32 devices in a mesh: sp: 16 (over z, y, x), tp: 2 (over core).
Axes of the slice: x: 2, y: 2, z: 4, core: 2. Of those that a mesh axis runs over, the one named last changes fastest.
Arguments:
- resid: bfloat16 [4096, 2048], P(('sp', 'tp')), may hold values from -6 to 6
- queries: bfloat16 [4096, 2048], P('sp', 'tp'), may hold values from -6 to 6
- keys: bfloat16 [4096, 1024], P('sp', 'tp'), may hold values from -6 to 6
- values: bfloat16 [4096, 1024], P('sp', 'tp'), may hold values from -6 to 6
- log_gates: float32 [16, 4096], P('tp'), as said below
- documents: int32 [4096], P('sp'), may hold values from 0 to 2, never falling along the last dimension, each value on 1 to 3072 neighbouring positions
- out_weight: bfloat16 [2048, 2048], P('tp'), may hold values from -0.125 to 0.125
- attn_gain: float32 [2048], replicated, may hold values from 0.1 to 1.9
- mlp_gain: float32 [2048], replicated, may hold values from 0.1 to 1.9
- gate_weight: bfloat16 [2048, 4096], P('sp', 'tp'), may hold values from -0.125 to 0.125
- up_weight: bfloat16 [2048, 4096], P('sp', 'tp'), may hold values from -0.125 to 0.125
- down_weight: bfloat16 [4096, 2048], P('tp', 'sp'), may hold values from -0.375 to 0.375
Outputs:
- mixed: bfloat16 [4096, 2048], P(('sp', 'tp'))
The draws below stay inside these ranges and needn't reach their ends.
Inputs may be any that keep to these rules, and one draw needn't show every extreme that they name: `log_gates`: each head's row never rises from one position to the next and starts at or below 0. `documents`: document numbers never fall along the positions; one document spans exactly three quarters of the 4096 positions.
All inputs are finite; a program needn't handle non-finite values.
Results may differ from the reference program's by a relative error of at most 0.018.
Values may be sent and summed in bfloat16 or wider, within the bound.
A program may use at most 64 MiB of HBM per device.

```python
import math
import jax
import jax.numpy as jnp
import numpy as np
from jax import lax

D = 2048
H = 16
KVH = 8
HD = 128
FF = 4096
TOKENS = 4096
ATT = 2048


def planted_pair(key):
    query_seed = jax.random.fold_in(key, 101)
    key_seed = jax.random.fold_in(key, 202)
    query_part = jnp.clip(jax.random.normal(query_seed, (TOKENS, H * HD), jnp.float32), -6.0, 6.0)
    key_part = jnp.clip(jax.random.normal(key_seed, (TOKENS, KVH * HD), jnp.float32), -6.0, 6.0)
    return (query_part, key_part)


def draw_queries(key, part):
    return planted_pair(key)[0].astype(jnp.bfloat16)


def draw_keys(key, part):
    return planted_pair(key)[1].astype(jnp.bfloat16)


def draw_log_gates(key, part):
    order_seed = jax.random.fold_in(key, 11)
    local_seed = jax.random.fold_in(key, 12)
    fast_seed = jax.random.fold_in(key, 13)
    slow_seed = jax.random.fold_in(key, 14)
    block_seed = jax.random.fold_in(key, 15)
    head_order = jax.random.permutation(order_seed, H)
    fast = head_order < H // 2
    local = jnp.exp(0.8 * jax.random.normal(local_seed, (H, TOKENS), jnp.float32))
    fast_rate = jnp.exp(jax.random.uniform(fast_seed, (H,), jnp.float32, math.log(1.0 / 150.0), math.log(1.0 / 45.0)))
    slow_rate = jnp.exp(jax.random.uniform(slow_seed, (H,), jnp.float32, math.log(0.3), math.log(1.2))) / TOKENS
    rate = jnp.where(fast, fast_rate, slow_rate)
    block_factor = jnp.exp(jax.random.uniform(block_seed, (H, TOKENS // 64), jnp.float32, math.log(0.5), math.log(2.0)))
    stretched = jnp.repeat(block_factor, 64, axis=1)
    return -jnp.cumsum(rate[:, None] * stretched * local, axis=1)


def block_levels(key, dims, split, smallest, top_value):
    level = 1.0
    for axis_at, blocks in split:
        steps = jax.random.uniform(jax.random.fold_in(jax.random.fold_in(key, 6), axis_at), (blocks,), jnp.float32, smallest / len(split), top_value / len(split))
        level = level * jnp.repeat(jnp.exp(steps), dims[axis_at] // blocks).reshape((-1,) + (1,) * (len(dims) - 1 - axis_at))
    return level


def length_profile(count, total, reach, lean):
    weights = [(1 << 20) // math.isqrt(standing ** lean) + 1 for standing in range(2, count + 1)]
    surplus, counts = total - reach - (count - 1), [1] * (count - 1)
    while surplus > 0:
        movable = [i for i in range(count - 1) if counts[i] < reach]
        mass, left = sum([weights[i] for i in movable]), surplus
        for i in movable:
            more = min(reach - counts[i], max(1, left * weights[i] // mass), surplus)
            counts[i] = counts[i] + more
            surplus = surplus - more
    return np.array([reach] + counts)


def ragged_sizes(own_key, count, total, limit, slope):
    if count == 2:
        one = jax.random.randint(own_key, (), max(1, total - limit), min(limit, total - 1) + 1)
        return jnp.stack([one, total - one])
    tallies = jnp.asarray(length_profile(count, total, limit, slope), jnp.int32)
    pairs = (count - 1) // 2
    giver, taker = tallies[1:1 + 2 * pairs:2], tallies[2:2 + 2 * pairs:2]
    slack = jnp.minimum(giver - 1, limit - taker)
    moved = jax.random.randint(jax.random.fold_in(own_key, 1), (pairs,), 0, 1 << 20) % (slack + 1)
    tallies = tallies.at[1:1 + 2 * pairs:2].set(giver - moved).at[2:2 + 2 * pairs:2].set(taker + moved)
    return tallies[jax.random.permutation(jax.random.fold_in(own_key, 2), count)]


def centred(rng, extent, spread, most, cuts=(), held_as=jnp.bfloat16):
    level = block_levels(rng, extent, cuts, -0.22, 0.18) if cuts else 1.0
    entries = jax.random.normal(rng, extent, jnp.float32) * spread * level
    return jnp.minimum(jnp.maximum(entries, -most), most).astype(held_as)


def setup_inputs(seed: int = 0) -> dict:
    splits = jax.random.split(jax.random.key(seed), 13)
    resid = centred(splits[0], (TOKENS, D), 1.0, 6.0, ((0, 32),))
    queries = draw_queries(jax.random.fold_in(splits[12], 71), 0)
    keys = draw_keys(jax.random.fold_in(splits[12], 71), 0)
    values = centred(splits[3], (TOKENS, KVH * HD), 1.0, 6.0, ((0, 16), (1, 2)))
    log_gates = draw_log_gates(jax.random.fold_in(splits[12], 71), 0)
    documents = jnp.searchsorted(jnp.cumsum(ragged_sizes(splits[5], 3, TOKENS, TOKENS * 3 // 4, 0)), jnp.arange(TOKENS), side="right").astype(jnp.int32)
    out_weight = centred(splits[6], (ATT, D), ATT ** -0.5, 0.125, ((0, 2),))
    attn_gain = jnp.clip(1.0 + 0.18 * jax.random.normal(splits[7], (D,), jnp.float32), 0.1, 1.9)
    mlp_gain = jnp.clip(1.0 + 0.18 * jax.random.normal(splits[8], (D,), jnp.float32), 0.1, 1.9)
    gate_weight = centred(splits[9], (D, FF), D ** -0.5, 0.125, ((0, 16), (1, 2)))
    up_weight = centred(splits[10], (D, FF), D ** -0.5, 0.125, ((0, 16), (1, 2)))
    down_weight = centred(splits[11], (FF, D), (FF // 16) ** -0.5, 0.375, ((0, 2), (1, 16)))
    return dict(resid=resid, queries=queries, keys=keys, values=values, log_gates=log_gates, documents=documents, out_weight=out_weight, attn_gain=attn_gain, mlp_gain=mlp_gain, gate_weight=gate_weight, up_weight=up_weight, down_weight=down_weight)


def reference(resid, queries, keys, values, log_gates, documents, out_weight, attn_gain, mlp_gain, gate_weight, up_weight, down_weight):
    group_size = H // KVH
    score_scale = 1.0 / math.sqrt(HD)
    key_heads = keys.reshape(TOKENS, KVH, HD).astype(jnp.float32)
    value_heads = values.reshape(TOKENS, KVH, HD).astype(jnp.float32)
    key_gates = log_gates.reshape(KVH, group_size, TOKENS)
    positions = jnp.arange(TOKENS, dtype=jnp.int32)
    block_len = math.gcd(TOKENS, 512)

    def attend(block_index):
        first_row = (block_index * block_len).astype(jnp.int32)
        query_block = lax.dynamic_slice_in_dim(queries, first_row, block_len, 0)
        query_block = query_block.reshape(block_len, KVH, group_size, HD).astype(jnp.float32)
        scores = jnp.einsum('tkgd,skd->kgts', query_block, key_heads) * score_scale
        query_gates = lax.dynamic_slice_in_dim(key_gates, first_row, block_len, 2)
        scores = scores + query_gates[..., None] - key_gates[:, :, None, :]
        query_pos = first_row + jnp.arange(block_len, dtype=jnp.int32)
        query_docs = lax.dynamic_slice_in_dim(documents, first_row, block_len, 0)
        visible = (positions[None, :] <= query_pos[:, None]) & (documents[None, :] == query_docs[:, None])
        scores = jnp.where(visible, scores, jnp.float32(-1e+30))
        row_max = lax.optimization_barrier(jnp.max(scores, axis=-1, keepdims=True))
        probs = jnp.where(visible, jnp.exp(scores - row_max), jnp.float32(0.0))
        row_sum = lax.optimization_barrier(jnp.sum(probs, axis=-1))
        probs_low = probs.astype(jnp.bfloat16).astype(jnp.float32)
        summed = jnp.einsum('kgts,skd->tkgd', probs_low, value_heads)
        summed = summed / jnp.transpose(row_sum, (2, 0, 1))[..., None]
        return summed.reshape(block_len, H * HD).astype(jnp.bfloat16)
    blocks = lax.map(attend, jnp.arange(TOKENS // block_len, dtype=jnp.int32))
    attended = blocks.reshape(TOKENS, H * HD)
    projected = jnp.dot(attended, out_weight, preferred_element_type=jnp.float32)
    power = lax.optimization_barrier(jnp.mean(projected * projected, axis=-1, keepdims=True))
    middle = resid.astype(jnp.float32) + attn_gain * projected * lax.rsqrt(power + 1e-06)
    middle_power = lax.optimization_barrier(jnp.mean(middle * middle, axis=-1, keepdims=True))
    normed = (mlp_gain * middle * lax.rsqrt(middle_power + 1e-06)).astype(jnp.bfloat16)
    gate_act = jnp.dot(normed, gate_weight, preferred_element_type=jnp.float32)
    up_act = jnp.dot(normed, up_weight, preferred_element_type=jnp.float32)
    hidden = (jax.nn.silu(gate_act) * up_act).astype(jnp.bfloat16)
    lowered = jnp.dot(hidden, down_weight, preferred_element_type=jnp.float32)
    return (middle + 0.5 * lowered).astype(jnp.bfloat16)
```

```python
import math

import jax
import jax.numpy as jnp
from jax import lax
from jax.experimental import pallas as pl
from jax.experimental.pallas import tpu as pltpu
from jax.sharding import PartitionSpec as P

HD = 128


def local(
    resid,
    queries,
    keys,
    values,
    log_gates,
    documents,
    out_weight,
    attn_gain,
    mlp_gain,
    gate_weight,
    up_weight,
    down_weight,
):
    tok_rows = queries.shape[0]
    kv_dev = keys.shape[1] // HD
    heads_dev = log_gates.shape[0]
    group_size = heads_dev // kv_dev
    score_scale = 1.0 / math.sqrt(HD)
    own_start = lax.axis_index("sp") * tok_rows
    own_last = own_start + tok_rows - 1
    first_doc = documents[0]
    query_pos = own_start + lax.iota(jnp.int32, tok_rows)
    query_heads = queries.reshape(tok_rows, kv_dev, group_size, HD)
    key_gates_all = log_gates.reshape(kv_dev, group_size, log_gates.shape[1])
    query_gates = lax.dynamic_slice_in_dim(key_gates_all, own_start, tok_rows, 2)
    collected = (
        lax.all_gather(gate_weight, "sp", axis=0, tiled=True),
        lax.all_gather(up_weight, "sp", axis=0, tiled=True),
        lax.all_gather(down_weight, "sp", axis=1, tiled=True),
    )
    residual_rows = resid.astype(jnp.float32)

    def attend_block(running, key_rows, value_rows, doc_rows, first_row):
        run_max, run_sum, accumulated = running
        key_count = key_rows.shape[0]
        scores = (
            jnp.einsum(
                "tkgd,skd->kgts",
                query_heads,
                key_rows.reshape(key_count, kv_dev, HD),
                preferred_element_type=jnp.float32,
            )
            * score_scale
        )
        key_gates = lax.dynamic_slice_in_dim(key_gates_all, first_row, key_count, 2)
        scores = scores + query_gates[..., None] - key_gates[:, :, None, :]
        key_pos = first_row + lax.iota(jnp.int32, key_count)
        visible = (key_pos[None, :] <= query_pos[:, None]) & (
            doc_rows[None, :] == documents[:, None]
        )
        scores = jnp.where(visible, scores, jnp.float32(-1e30))
        new_max = jnp.maximum(run_max, jnp.max(scores, axis=-1))
        probs = jnp.where(visible, jnp.exp(scores - new_max[..., None]), jnp.float32(0.0))
        shrink = jnp.exp(run_max - new_max)
        run_sum = run_sum * shrink + jnp.sum(probs, axis=-1)
        weighted = jnp.einsum(
            "kgts,skd->kgtd",
            probs.astype(jnp.bfloat16),
            value_rows.reshape(key_count, kv_dev, HD),
            preferred_element_type=jnp.float32,
        )
        accumulated = accumulated * shrink[..., None] + weighted
        return (new_max, run_sum, accumulated)

    def maybe_attend(running, key_rows, value_rows, doc_rows, first_row):
        needed = (first_row <= own_last) & (doc_rows[-1] >= first_doc)

        def compute(state):
            return attend_block(state, key_rows, value_rows, doc_rows, first_row)

        def keep(state):
            return state

        return lax.cond(needed, compute, keep, running)

    start_state = (
        jnp.full((kv_dev, group_size, tok_rows), -1e30, jnp.float32),
        jnp.zeros((kv_dev, group_size, tok_rows), jnp.float32),
        jnp.zeros((kv_dev, group_size, tok_rows, HD), jnp.float32),
    )
    key_rows = lax.all_gather(keys, "sp", axis=0, tiled=True)
    value_rows = lax.all_gather(values, "sp", axis=0, tiled=True)
    doc_rows = lax.all_gather(documents, "sp", axis=0, tiled=True)
    key_count = key_rows.shape[0]
    block_len = math.gcd(key_count, 1024)

    def advance(block_index, inner):
        offset = block_index * block_len
        return maybe_attend(
            inner,
            lax.dynamic_slice_in_dim(key_rows, offset, block_len, 0),
            lax.dynamic_slice_in_dim(value_rows, offset, block_len, 0),
            lax.dynamic_slice_in_dim(doc_rows, offset, block_len, 0),
            offset,
        )

    run_max, run_sum, accumulated = lax.fori_loop(0, key_count // block_len, advance, start_state)
    attended = accumulated / run_sum[..., None]
    attended = (
        jnp.transpose(attended, (2, 0, 1, 3)).reshape(tok_rows, heads_dev * HD).astype(jnp.bfloat16)
    )
    rows_slice = attended
    projected = lax.psum_scatter(
        jnp.dot(rows_slice, out_weight, preferred_element_type=jnp.float32).astype(jnp.bfloat16),
        "tp",
        scatter_dimension=0,
        tiled=True,
    ).astype(jnp.float32)
    power = jnp.mean(projected * projected, axis=-1, keepdims=True)
    middle = residual_rows + attn_gain * projected * lax.rsqrt(power + 1e-06)
    middle_power = jnp.mean(middle * middle, axis=-1, keepdims=True)
    normed = (mlp_gain * middle * lax.rsqrt(middle_power + 1e-06)).astype(jnp.bfloat16)
    normed_all = lax.all_gather(normed, "tp", axis=0, tiled=True)
    gate_full, up_full, down_full = collected
    gate_act = jnp.dot(normed_all, gate_full, preferred_element_type=jnp.float32)
    up_act = jnp.dot(normed_all, up_full, preferred_element_type=jnp.float32)
    hidden = (jax.nn.silu(gate_act) * up_act).astype(jnp.bfloat16)
    rows_slice = hidden
    lowered = lax.psum_scatter(
        jnp.dot(rows_slice, down_full, preferred_element_type=jnp.float32).astype(jnp.bfloat16),
        "tp",
        scatter_dimension=0,
        tiled=True,
    ).astype(jnp.float32)
    return (middle + 0.5 * lowered).astype(jnp.bfloat16)


GROUP = 4
PLANE = 4
MESH = pl.DeviceIdType.MESH
LOG2E = 1.4426950408889634
VMEM = pl.BlockSpec(memory_space=pltpu.VMEM)
K, V, DOC, GATE, UP, DOWN, Q = range(7)


def remote(src, dst, send_sem, recv_sem, target):
    return pltpu.make_async_remote_copy(
        src_ref=src,
        dst_ref=dst,
        send_sem=send_sem,
        recv_sem=recv_sem,
        device_id=target,
        device_id_type=MESH,
    )


def span(index, width):
    return pl.ds(pl.multiple_of(index * width, width), width)


def layer_kernel(
    q_ref, k_ref, v_ref, d_ref, lg_ref, ow_ref, resid_ref, ag_ref, mg_ref, g_ref, u_ref, w_ref,
    out_ref,
    kall, vall, docs, qs, gkc, gw, uw, dw, att, arr, pbuf, pgot, mid, nall, hid, part, pair, red,
    got,
    z_send, z_recv, p_send, p_recv, own_sem, a_send, a_recv, t_send, t_recv,
    o_send, n_send, n_recv, f_send, f_recv, x_send, x_recv, r_send, r_recv,
):
    me = lax.axis_index("sp")
    core = lax.axis_index("tp")
    z, p = me // PLANE, me % PLANE
    px, py = p % 2, p // 2
    other = 1 - core
    mate = (me, other)
    rows = k_ref.shape[0]
    qcols = q_ref.shape[1] // GROUP
    rank = qcols // HD
    fcols = g_ref.shape[1] // GROUP
    wrows, wcols = g_ref.shape[0], w_ref.shape[1]
    half, d_model = resid_ref.shape
    coef = LOG2E / math.sqrt(HD)
    neighbours = (1, 2, 3)

    def peer(e):
        x = px if e == 2 else 1 - px
        y = py if e == 1 else 1 - py
        return y * 2 + x

    def near(e):
        return (z * PLANE + peer(e), core)

    def there(zb):
        return (zb * PLANE + p, core)

    def place(a, k):
        if a == K:
            return kall.at[span(k, rows)]
        if a == V:
            return vall.at[span(k, rows)]
        if a == DOC:
            return docs.at[k]
        if a == GATE:
            return gw.at[span(k, wrows)]
        if a == UP:
            return uw.at[span(k, wrows)]
        if a == DOWN:
            return dw.at[:, span(k, wcols)]
        return qs.at[k // PLANE]

    def piece(a, to):
        if a == K:
            return k_ref.at[:, span(to, HD)]
        if a == V:
            return v_ref.at[:, span(to, HD)]
        if a == DOC:
            return d_ref.at[...]
        if a == GATE:
            return g_ref.at[:, span(to, fcols)]
        if a == UP:
            return u_ref.at[:, span(to, fcols)]
        if a == DOWN:
            return w_ref.at[span(to, fcols)]
        return q_ref.at[:, span(to, qcols)]

    barrier = pltpu.get_barrier_semaphore()
    for d in range(1, GROUP):
        pl.semaphore_signal(barrier, inc=1, device_id=there((z + d) % GROUP), device_id_type=MESH)
    for e in neighbours:
        pl.semaphore_signal(barrier, inc=1, device_id=near(e), device_id_type=MESH)
    pl.semaphore_signal(barrier, inc=1, device_id=mate, device_id_type=MESH)
    pl.semaphore_wait(barrier, 7)

    def z_copy(a, to):
        return remote(piece(a, to), place(a, me), z_send.at[a, to], z_recv.at[a, z], there(to))

    def z_sends(a):
        for d in (1, 3, 2):
            z_copy(a, (z + d) % GROUP).start()

    def z_arrival(a, zs):
        at = place(a, zs * PLANE + p)
        remote(at, at, z_send.at[a, z], z_recv.at[a, zs], mate).wait_recv()

    def own_copy(a):
        return pltpu.make_async_copy(piece(a, z), place(a, me), own_sem.at[a])

    def p_copy(a, zs, e):
        at = place(a, zs * PLANE + p)
        return remote(at, at, p_send.at[a, zs, e - 1], p_recv.at[a, zs, e - 1], near(e))

    def p_own(a, e):
        return remote(piece(a, z), place(a, me), p_send.at[a, z, e - 1], p_recv.at[a, z, e - 1],
                      near(e))

    def p_arrival(a, zs, e):
        at = place(a, zs * PLANE + peer(e))
        remote(at, at, p_send.at[a, zs, e - 1], p_recv.at[a, zs, e - 1], mate).wait_recv()

    def spread_own(a):
        for e in neighbours:
            p_own(a, e).start()

    def forward(a, zs):
        z_arrival(a, zs)
        for e in neighbours:
            p_copy(a, zs, e).start()

    for a in (DOC, K, V, Q, GATE):
        z_sends(a)
    for a in (DOC, K, V, GATE):
        spread_own(a)
    for a in range(7):
        own_copy(a).start()

    lanes = 128

    @pl.loop(0, kall.shape[0] // lanes)
    def _(j):
        at = span(j, lanes)
        for r in range(rank):
            row = lg_ref[z, r:r + 1, at] * LOG2E
            gkc[r, at, :] = jnp.transpose(jnp.broadcast_to(row, (lanes, lanes)))

    def ascending(i):
        return i + (i - z + GROUP) // GROUP

    @pl.loop(0, GROUP - 1)
    def _(i):
        forward(DOC, ascending(i))

    @pl.loop(0, GROUP - 1)
    def _(i):
        forward(K, ascending(i))
        forward(V, ascending(i))

    spread_own(UP)
    spread_own(DOWN)
    for a in range(7):
        own_copy(a).wait()
    for d in range(1, GROUP):
        z_arrival(Q, (z + d) % GROUP)

    @pl.loop(0, GROUP)
    def _(zs):
        for e in neighbours:
            p_arrival(DOC, zs, e)

    every_doc = docs[...]

    def below(level):
        total = jnp.sum((every_doc < level).astype(jnp.float32), axis=0)
        return jnp.sum(total, axis=1, keepdims=True)

    first_of_1, first_of_2 = below(1), below(2)

    @pl.loop(0, GROUP)
    def _(zq):
        for e in neighbours:
            p_arrival(K, zq, e)
            p_arrival(V, zq, e)
        block = zq * PLANE + p
        q = jnp.concatenate([qs[zq, :, r * HD:(r + 1) * HD] for r in range(rank)], axis=0)
        own = span(block, rows)
        gq = jnp.concatenate([lg_ref[z, r:r + 1, own] for r in range(rank)], axis=1) * LOG2E
        dq = docs[block]
        start = jnp.where(dq == 0, 0.0, jnp.where(dq == 1, first_of_1, first_of_2))
        start = jnp.concatenate([start.astype(jnp.int32)] * rank, axis=1)
        qpos = block * rows + lax.broadcasted_iota(jnp.int32, (1, rows), 1)
        qpos = jnp.concatenate([qpos] * rank, axis=1)

        def attend(base, count, causal, state):
            m, l, acc = state
            at = pl.ds(pl.multiple_of(base, count), count)
            s = lax.dot_general(kall[at], q, (((1,), (1,)), ((), ())),
                                preferred_element_type=jnp.float32)
            gk = jnp.concatenate(
                [gkc[r, at, :] for r in range(rank) for _ in range(rows // lanes)], axis=1)
            s = (s * coef + gq) - gk
            kpos = base + lax.broadcasted_iota(jnp.int32, (count, 1), 0)
            seen = kpos >= start
            if causal:
                seen = seen & (kpos <= qpos)
            s = jnp.where(seen, s, jnp.float32(-1e30))
            m_new = jnp.maximum(m, jnp.max(s, axis=0, keepdims=True))
            prob = jnp.exp2(s - m_new)
            shrink = jnp.exp2(m - m_new)
            l = l * shrink + jnp.sum(prob, axis=0, keepdims=True)
            acc = acc * shrink + lax.dot_general(
                vall[at], prob.astype(jnp.bfloat16), (((0,), (0,)), ((), ())),
                preferred_element_type=jnp.float32)
            return m_new, l, acc

        wide = 2 * rows
        state = (jnp.full((1, rank * rows), -1e20, jnp.float32),
                 jnp.zeros((1, rank * rows), jnp.float32),
                 jnp.zeros((HD, rank * rows), jnp.float32))
        state = lax.fori_loop(0, 2 * zq, lambda i, s: attend(i * wide, wide, False, s), state)
        m, l, acc = lax.fori_loop(
            0, p + 1, lambda i, s: attend((zq * PLANE + i) * rows, rows, True, s), state)
        res = acc / l
        for r in range(rank):
            att[zq, :, r * HD:(r + 1) * HD] = jnp.transpose(
                res[:, r * rows:(r + 1) * rows]).astype(jnp.bfloat16)

        @pl.when(zq != z)
        def _():
            remote(att.at[zq], arr.at[z], a_send.at[zq], a_recv.at[z], there(zq)).start()

        @pl.when(zq == 0)
        def _():
            z_sends(UP)

    own = pltpu.make_async_copy(att.at[z], arr.at[z], own_sem.at[0])
    own.start()
    own.wait()
    for d in range(1, GROUP):
        zs = (z + d) % GROUP
        at = arr.at[zs]
        remote(at, at, a_send.at[zs], a_recv.at[zs], mate).wait_recv()
    tile = 512

    @pl.loop(0, d_model // tile)
    def _(j):
        at = span(j, tile)
        total = jnp.dot(arr[0], ow_ref[0:qcols, at], preferred_element_type=jnp.float32)
        for g in range(1, GROUP):
            total += jnp.dot(arr[g], ow_ref[g * qcols:(g + 1) * qcols, at],
                             preferred_element_type=jnp.float32)
        pbuf[0, :, at] = total[:half].astype(jnp.bfloat16)
        pbuf[1, :, at] = total[half:].astype(jnp.bfloat16)

    swap = remote(pbuf.at[other], pgot, t_send, t_recv, mate)
    swap.start()
    swap.wait()
    projected = pbuf[core].astype(jnp.float32) + pgot[...].astype(jnp.float32)
    power = jnp.mean(projected * projected, axis=-1, keepdims=True)
    middle = resid_ref[...].astype(jnp.float32) + ag_ref[...] * projected * lax.rsqrt(power + 1e-06)
    mid[...] = middle
    mpower = jnp.mean(middle * middle, axis=-1, keepdims=True)
    nall[z, core] = (mg_ref[...] * middle * lax.rsqrt(mpower + 1e-06)).astype(jnp.bfloat16)

    def relay(zb, side, send_sem):
        block = nall.at[zb, core]
        return remote(block, block, send_sem, n_recv.at[zb],
                      ((z + 1 - 2 * side) * PLANE + p, core))

    def share(zb):
        block = nall.at[zb, core]
        return remote(block, block, f_send.at[zb], f_recv.at[zb], mate)

    def onward(side):
        return (side == 0) & (z < GROUP - 1) | (side == 1) & (z > 0)

    for side in (0, 1):
        @pl.when(onward(side))
        def _():
            relay(z, side, o_send.at[side]).start()
    share(z).start()
    z_sends(DOWN)

    def arrive(d):
        for side in (0, 1):
            zb = z - d if side == 0 else z + d

            @pl.when((zb >= 0) & (zb < GROUP))
            def _():
                block = nall.at[zb, core]
                remote(block, block, n_send.at[zb], n_recv.at[zb], mate).wait_recv()
                @pl.when(onward(side))
                def _():
                    relay(zb, side, n_send.at[zb]).start()
                share(zb).start()

    def forwards(a):
        for d in (1, 3, 2):
            forward(a, (z + d) % GROUP)

    forwards(GATE)
    forwards(UP)
    arrive(1)
    arrive(2)
    forwards(DOWN)
    arrive(3)

    @pl.loop(0, GROUP)
    def _(zs):
        for a in (GATE, UP):
            for e in neighbours:
                p_arrival(a, zs, e)

    @pl.loop(0, GROUP)
    def _(i):
        zb = (z + i) % GROUP
        over = nall.at[zb, other]
        remote(over, over, f_send.at[zb], f_recv.at[zb], mate).wait_recv()
        rows_in = jnp.concatenate([nall[zb, 0], nall[zb, 1]], axis=0)
        ftile = 256
        for j in range(fcols // ftile):
            at = slice(j * ftile, (j + 1) * ftile)
            gate = jnp.dot(rows_in, gw[:, at], preferred_element_type=jnp.float32)
            up = jnp.dot(rows_in, uw[:, at], preferred_element_type=jnp.float32)
            hid[zb, :, at] = (gate / (1.0 + jnp.exp(-gate)) * up).astype(jnp.bfloat16)

    gcols = PLANE * wcols

    def trade(zb, g):
        at = span(g, gcols)
        return remote(part.at[zb, other, :, at], pair.at[zb, :, at], x_send.at[zb, g],
                      x_recv.at[zb, g], mate)

    def give(zb, g):
        at = span(g, gcols)
        return remote(red.at[zb, :, at], got.at[z, :, at], r_send.at[zb, g], r_recv.at[z, g],
                      there(zb))

    def take(zb, g):
        at = span(g, gcols)
        remote(red.at[zb, :, at], got.at[zb, :, at], r_send.at[zb, g], r_recv.at[zb, g],
               mate).wait_recv()

    @pl.loop(0, GROUP)
    def _(i):
        g = (z + i) % GROUP
        at = span(g, gcols)
        for e in neighbours:
            p_arrival(DOWN, g, e)

        @pl.loop(1, GROUP + 1)
        def _(d):
            zb = (z + d) % GROUP
            total = jnp.dot(hid[zb], dw[:, at], preferred_element_type=jnp.float32)
            part[zb, 0, :, at] = total[:half].astype(jnp.bfloat16)
            part[zb, 1, :, at] = total[half:].astype(jnp.bfloat16)
            trade(zb, g).start()

        @pl.loop(1, GROUP)
        def _(d):
            zb = (z + d) % GROUP
            trade(zb, g).wait()
            red[zb, :, at] = (part[zb, core, :, at].astype(jnp.float32)
                              + pair[zb, :, at].astype(jnp.float32)).astype(jnp.bfloat16)
            give(zb, g).start()
        trade(z, g).wait()

    @pl.loop(0, GROUP)
    def _(i):
        g = (z + i) % GROUP
        for d in range(1, GROUP):
            take((z + d) % GROUP, (g + GROUP - d) % GROUP)

    @pl.loop(0, GROUP)
    def _(g):
        at = span(g, gcols)
        total = part[z, core, :, at].astype(jnp.float32) + pair[z, :, at].astype(jnp.float32)
        for d in range(1, GROUP):
            total += got[(z + d) % GROUP, :, at].astype(jnp.float32)
        out_ref[:, at] = (mid[:, at] + 0.5 * total).astype(jnp.bfloat16)

    for d in range(1, GROUP):
        zb = (z + d) % GROUP
        for a in range(7):
            z_copy(a, zb).wait_send()
        remote(att.at[zb], arr.at[z], a_send.at[zb], a_recv.at[z], there(zb)).wait_send()

        @pl.loop(0, GROUP)
        def _(g):
            give(zb, g).wait_send()
    for a in range(6):
        for e in neighbours:
            p_own(a, e).wait_send()
            for d in range(1, GROUP):
                p_copy(a, (z + d) % GROUP, e).wait_send()
    share(z).wait_send()
    for side in (0, 1):
        @pl.when(onward(side))
        def _():
            relay(z, side, o_send.at[side]).wait_send()
    for d in range(1, GROUP):
        share((z + d) % GROUP).wait_send()
        for side in (0, 1):
            zb = z - d if side == 0 else z + d

            @pl.when((zb >= 0) & (zb < GROUP) & onward(side))
            def _():
                relay(zb, side, n_send.at[zb]).wait_send()


def grouped(
    sp, resid, queries, keys, values, log_gates, documents, out_weight, attn_gain, mlp_gain,
    gate_weight, up_weight, down_weight,
):
    rows, ff = keys.shape[0], gate_weight.shape[1] // GROUP
    half, d_model = resid.shape
    tokens = rows * sp
    qcols = queries.shape[1] // GROUP
    rank = qcols // HD
    bf, f32 = jnp.bfloat16, jnp.float32
    dma = pltpu.SemaphoreType.DMA
    return pl.pallas_call(
        layer_kernel,
        out_shape=jax.ShapeDtypeStruct(resid.shape, bf),
        in_specs=[VMEM] * 12,
        out_specs=VMEM,
        scratch_shapes=[
            pltpu.VMEM((tokens, HD), bf),
            pltpu.VMEM((tokens, HD), bf),
            pltpu.VMEM((sp, 1, rows), jnp.int32),
            pltpu.VMEM((GROUP, rows, qcols), bf),
            pltpu.VMEM((rank, tokens, 128), f32),
            pltpu.VMEM((d_model, ff), bf),
            pltpu.VMEM((d_model, ff), bf),
            pltpu.VMEM((ff, d_model), bf),
            pltpu.VMEM((GROUP, rows, qcols), bf),
            pltpu.VMEM((GROUP, rows, qcols), bf),
            pltpu.VMEM((2, half, d_model), bf),
            pltpu.VMEM((half, d_model), bf),
            pltpu.VMEM((half, d_model), f32),
            pltpu.VMEM((GROUP, 2, half, d_model), bf),
            pltpu.VMEM((GROUP, rows, ff), bf),
            pltpu.VMEM((GROUP, 2, half, d_model), bf),
            pltpu.VMEM((GROUP, half, d_model), bf),
            pltpu.VMEM((GROUP, half, d_model), bf),
            pltpu.VMEM((GROUP, half, d_model), bf),
            dma((7, GROUP)), dma((7, GROUP)), dma((6, GROUP, 3)), dma((6, GROUP, 3)), dma((7,)),
            dma((GROUP,)), dma((GROUP,)), dma, dma,
            dma((2,)), dma((GROUP,)), dma((GROUP,)), dma((GROUP,)), dma((GROUP,)),
            dma((GROUP, GROUP)), dma((GROUP, GROUP)), dma((GROUP, GROUP)), dma((GROUP, GROUP)),
        ],
        compiler_params=pltpu.CompilerParams(
            collective_id=0, has_side_effects=True, vmem_limit_bytes=62 * 1024 * 1024),
    )(queries, keys, values, documents[None, :], log_gates.reshape(GROUP, rank, tokens),
      out_weight, resid, attn_gain[None, :], mlp_gain[None, :], gate_weight, up_weight,
      down_weight)


def solution(mesh):
    placed = (
        P(("sp", "tp"), None),
        P("sp", "tp"),
        P("sp", "tp"),
        P("sp", "tp"),
        P("tp", None),
        P("sp"),
        P("tp", None),
        P(),
        P(),
        P("sp", "tp"),
        P("sp", "tp"),
        P("tp", "sp"),
    )
    sp, tp = mesh.shape["sp"], mesh.shape["tp"]

    def layer(*args):
        kv_dev = args[2].shape[1] // HD
        fits = tp == 2 and sp == GROUP * PLANE and kv_dev == GROUP
        return grouped(sp, *args) if fits else local(*args)

    return jax.shard_map(
        layer, mesh=mesh, in_specs=placed, out_specs=P(("sp", "tp"), None), check_vma=False
    )
```

```python
import math

import jax
import jax.numpy as jnp
from jax import lax
from jax.experimental import pallas as pl
from jax.experimental.pallas import tpu as pltpu
from jax.sharding import PartitionSpec as P

HD = 128


def local(
    resid,
    queries,
    keys,
    values,
    log_gates,
    documents,
    out_weight,
    attn_gain,
    mlp_gain,
    gate_weight,
    up_weight,
    down_weight,
):
    tok_rows = queries.shape[0]
    kv_dev = keys.shape[1] // HD
    heads_dev = log_gates.shape[0]
    group_size = heads_dev // kv_dev
    score_scale = 1.0 / math.sqrt(HD)
    own_start = lax.axis_index("sp") * tok_rows
    own_last = own_start + tok_rows - 1
    first_doc = documents[0]
    query_pos = own_start + lax.iota(jnp.int32, tok_rows)
    query_heads = queries.reshape(tok_rows, kv_dev, group_size, HD)
    key_gates_all = log_gates.reshape(kv_dev, group_size, log_gates.shape[1])
    query_gates = lax.dynamic_slice_in_dim(key_gates_all, own_start, tok_rows, 2)
    collected = (
        lax.all_gather(gate_weight, "sp", axis=0, tiled=True),
        lax.all_gather(up_weight, "sp", axis=0, tiled=True),
        lax.all_gather(down_weight, "sp", axis=1, tiled=True),
    )
    residual_rows = resid.astype(jnp.float32)

    def attend_block(running, key_rows, value_rows, doc_rows, first_row):
        run_max, run_sum, accumulated = running
        key_count = key_rows.shape[0]
        scores = (
            jnp.einsum(
                "tkgd,skd->kgts",
                query_heads,
                key_rows.reshape(key_count, kv_dev, HD),
                preferred_element_type=jnp.float32,
            )
            * score_scale
        )
        key_gates = lax.dynamic_slice_in_dim(key_gates_all, first_row, key_count, 2)
        scores = scores + query_gates[..., None] - key_gates[:, :, None, :]
        key_pos = first_row + lax.iota(jnp.int32, key_count)
        visible = (key_pos[None, :] <= query_pos[:, None]) & (
            doc_rows[None, :] == documents[:, None]
        )
        scores = jnp.where(visible, scores, jnp.float32(-1e30))
        new_max = jnp.maximum(run_max, jnp.max(scores, axis=-1))
        probs = jnp.where(visible, jnp.exp(scores - new_max[..., None]), jnp.float32(0.0))
        shrink = jnp.exp(run_max - new_max)
        run_sum = run_sum * shrink + jnp.sum(probs, axis=-1)
        weighted = jnp.einsum(
            "kgts,skd->kgtd",
            probs.astype(jnp.bfloat16),
            value_rows.reshape(key_count, kv_dev, HD),
            preferred_element_type=jnp.float32,
        )
        accumulated = accumulated * shrink[..., None] + weighted
        return (new_max, run_sum, accumulated)

    def maybe_attend(running, key_rows, value_rows, doc_rows, first_row):
        needed = (first_row <= own_last) & (doc_rows[-1] >= first_doc)

        def compute(state):
            return attend_block(state, key_rows, value_rows, doc_rows, first_row)

        def keep(state):
            return state

        return lax.cond(needed, compute, keep, running)

    start_state = (
        jnp.full((kv_dev, group_size, tok_rows), -1e30, jnp.float32),
        jnp.zeros((kv_dev, group_size, tok_rows), jnp.float32),
        jnp.zeros((kv_dev, group_size, tok_rows, HD), jnp.float32),
    )
    key_rows = lax.all_gather(keys, "sp", axis=0, tiled=True)
    value_rows = lax.all_gather(values, "sp", axis=0, tiled=True)
    doc_rows = lax.all_gather(documents, "sp", axis=0, tiled=True)
    key_count = key_rows.shape[0]
    block_len = math.gcd(key_count, 1024)

    def advance(block_index, inner):
        offset = block_index * block_len
        return maybe_attend(
            inner,
            lax.dynamic_slice_in_dim(key_rows, offset, block_len, 0),
            lax.dynamic_slice_in_dim(value_rows, offset, block_len, 0),
            lax.dynamic_slice_in_dim(doc_rows, offset, block_len, 0),
            offset,
        )

    run_max, run_sum, accumulated = lax.fori_loop(0, key_count // block_len, advance, start_state)
    attended = accumulated / run_sum[..., None]
    attended = (
        jnp.transpose(attended, (2, 0, 1, 3)).reshape(tok_rows, heads_dev * HD).astype(jnp.bfloat16)
    )
    rows_slice = attended
    projected = lax.psum_scatter(
        jnp.dot(rows_slice, out_weight, preferred_element_type=jnp.float32).astype(jnp.bfloat16),
        "tp",
        scatter_dimension=0,
        tiled=True,
    ).astype(jnp.float32)
    power = jnp.mean(projected * projected, axis=-1, keepdims=True)
    middle = residual_rows + attn_gain * projected * lax.rsqrt(power + 1e-06)
    middle_power = jnp.mean(middle * middle, axis=-1, keepdims=True)
    normed = (mlp_gain * middle * lax.rsqrt(middle_power + 1e-06)).astype(jnp.bfloat16)
    normed_all = lax.all_gather(normed, "tp", axis=0, tiled=True)
    gate_full, up_full, down_full = collected
    gate_act = jnp.dot(normed_all, gate_full, preferred_element_type=jnp.float32)
    up_act = jnp.dot(normed_all, up_full, preferred_element_type=jnp.float32)
    hidden = (jax.nn.silu(gate_act) * up_act).astype(jnp.bfloat16)
    rows_slice = hidden
    lowered = lax.psum_scatter(
        jnp.dot(rows_slice, down_full, preferred_element_type=jnp.float32).astype(jnp.bfloat16),
        "tp",
        scatter_dimension=0,
        tiled=True,
    ).astype(jnp.float32)
    return (middle + 0.5 * lowered).astype(jnp.bfloat16)


GROUP = 4
PLANE = 4
MESH = pl.DeviceIdType.MESH
LOG2E = 1.4426950408889634
VMEM = pl.BlockSpec(memory_space=pltpu.VMEM)
ANY = pl.BlockSpec(memory_space=pl.ANY)
K, V, DOC, GATE, UP, DOWN, Q = range(7)


def remote(src, dst, send_sem, recv_sem, target):
    return pltpu.make_async_remote_copy(
        src_ref=src,
        dst_ref=dst,
        send_sem=send_sem,
        recv_sem=recv_sem,
        device_id=target,
        device_id_type=MESH,
    )


def span(index, width):
    return pl.ds(pl.multiple_of(index * width, width), width)


def layer_kernel(
    q_ref, k_ref, v_ref, d_ref, lg_ref, ow_hbm, resid_hbm, ag_ref, mg_ref, g_ref, u_ref, w_ref,
    out_ref,
    ow_ref, resid_ref,
    kall, vall, docs, qs, gkc, gw, uw, dw, att, arr, pbuf, pgot, mid, nall, hid, part, pair, red,
    got, comb,
    z_send, z_recv, p_send, p_recv, own_sem, load_sem, a_send, a_recv, t_send, t_recv,
    o_send, n_send, n_recv, f_send, f_recv, x_send, x_recv, r_send, r_recv, c_recv,
):
    me = lax.axis_index("sp")
    core = lax.axis_index("tp")
    z, p = me // PLANE, me % PLANE
    px, py = p % 2, p // 2
    other = 1 - core
    mate = (me, other)
    rows = k_ref.shape[0]
    qcols = q_ref.shape[1] // GROUP
    rank = qcols // HD
    fcols = g_ref.shape[1] // GROUP
    wrows, wcols = g_ref.shape[0], w_ref.shape[1]
    half, d_model = resid_hbm.shape
    coef = LOG2E / math.sqrt(HD)
    neighbours = (1, 2, 3)

    def peer(e):
        x = px if e == 2 else 1 - px
        y = py if e == 1 else 1 - py
        return y * 2 + x

    def near(e):
        return (z * PLANE + peer(e), core)

    def there(zb):
        return (zb * PLANE + p, core)

    def place(a, k):
        if a == K:
            return kall.at[span(k, rows)]
        if a == V:
            return vall.at[span(k, rows)]
        if a == DOC:
            return docs.at[k]
        if a == GATE:
            return gw.at[span(k, wrows)]
        if a == UP:
            return uw.at[span(k, wrows)]
        if a == DOWN:
            return dw.at[:, span(k, wcols)]
        return qs.at[k // PLANE]

    def piece(a, to):
        if a == K:
            return k_ref.at[:, span(to, HD)]
        if a == V:
            return v_ref.at[:, span(to, HD)]
        if a == DOC:
            return d_ref.at[...]
        if a == GATE:
            return g_ref.at[:, span(to, fcols)]
        if a == UP:
            return u_ref.at[:, span(to, fcols)]
        if a == DOWN:
            return w_ref.at[span(to, fcols)]
        return q_ref.at[:, span(to, qcols)]

    barrier = pltpu.get_barrier_semaphore()
    for d in range(1, GROUP):
        pl.semaphore_signal(barrier, inc=1, device_id=there((z + d) % GROUP), device_id_type=MESH)
    loads = (pltpu.make_async_copy(ow_hbm, ow_ref, load_sem.at[0]),
             pltpu.make_async_copy(resid_hbm, resid_ref, load_sem.at[1]))
    for e in neighbours:
        pl.semaphore_signal(barrier, inc=1, device_id=near(e), device_id_type=MESH)
    pl.semaphore_signal(barrier, inc=1, device_id=mate, device_id_type=MESH)
    pl.semaphore_wait(barrier, 7)

    def z_copy(a, to):
        return remote(piece(a, to), place(a, me), z_send.at[a, to], z_recv.at[a, z], there(to))

    def z_sends(a):
        for d in (1, 3, 2):
            z_copy(a, (z + d) % GROUP).start()

    def z_arrival(a, zs):
        at = place(a, zs * PLANE + p)
        remote(at, at, z_send.at[a, z], z_recv.at[a, zs], mate).wait_recv()

    def own_copy(a):
        return pltpu.make_async_copy(piece(a, z), place(a, me), own_sem.at[a])

    def p_copy(a, zs, e):
        at = place(a, zs * PLANE + p)
        return remote(at, at, p_send.at[a, zs, e - 1], p_recv.at[a, zs, e - 1], near(e))

    def p_own(a, e):
        return remote(piece(a, z), place(a, me), p_send.at[a, z, e - 1], p_recv.at[a, z, e - 1],
                      near(e))

    def p_arrival(a, zs, e):
        at = place(a, zs * PLANE + peer(e))
        remote(at, at, p_send.at[a, zs, e - 1], p_recv.at[a, zs, e - 1], mate).wait_recv()

    def spread_own(a):
        for e in neighbours:
            p_own(a, e).start()

    def forward(a, zs):
        z_arrival(a, zs)
        for e in neighbours:
            p_copy(a, zs, e).start()

    for a in (DOC, K, V, Q, GATE):
        z_sends(a)
    for a in (DOC, K, V):
        spread_own(a)
    for a in range(7):
        own_copy(a).start()
    for load in loads:
        load.start()

    lanes = 128

    def gate_row(r, at):
        block = lg_ref[:, at]
        chosen = lax.broadcasted_iota(jnp.int32, block.shape, 0) == z * rank + r
        return jnp.sum(jnp.where(chosen, block, 0.0), axis=0, keepdims=True) * LOG2E

    @pl.loop(0, kall.shape[0] // lanes)
    def _(j):
        at = span(j, lanes)
        for r in range(rank):
            row = gate_row(r, at)
            gkc[r, at, :] = jnp.transpose(jnp.broadcast_to(row, (lanes, lanes)))

    def ascending(i):
        return i + (i - z + GROUP) // GROUP

    @pl.loop(0, GROUP - 1)
    def _(i):
        forward(DOC, ascending(i))

    @pl.loop(0, GROUP - 2)
    def _(i):
        forward(K, ascending(i))
        forward(V, ascending(i))

    for a in range(7):
        own_copy(a).wait()

    @pl.loop(0, GROUP)
    def _(zs):
        for e in neighbours:
            p_arrival(DOC, zs, e)

    every_doc = docs[...]

    def below(level):
        total = jnp.sum((every_doc < level).astype(jnp.float32), axis=0)
        return jnp.sum(total, axis=1, keepdims=True)

    first_of_1, first_of_2 = below(1), below(2)

    @pl.loop(0, GROUP)
    def _(zq):
        @pl.when(zq == 1)
        def _():
            forward(K, ascending(GROUP - 2))
            forward(V, ascending(GROUP - 2))
            spread_own(GATE)
            spread_own(UP)

        @pl.when(zq != z)
        def _():
            z_arrival(Q, zq)

        for e in neighbours:
            p_arrival(K, zq, e)
            p_arrival(V, zq, e)
        block = zq * PLANE + p
        q = jnp.concatenate([qs[zq, :, r * HD:(r + 1) * HD] for r in range(rank)], axis=0)
        own = span(block, rows)
        gq = jnp.concatenate([gate_row(r, own) for r in range(rank)], axis=1)
        dq = docs[block]
        start = jnp.where(dq == 0, 0.0, jnp.where(dq == 1, first_of_1, first_of_2))
        start = jnp.concatenate([start.astype(jnp.int32)] * rank, axis=1)
        qpos = block * rows + lax.broadcasted_iota(jnp.int32, (1, rows), 1)
        qpos = jnp.concatenate([qpos] * rank, axis=1)

        def attend(base, count, causal, state):
            m, l, acc = state
            at = pl.ds(pl.multiple_of(base, count), count)
            s = lax.dot_general(kall[at], q, (((1,), (1,)), ((), ())),
                                preferred_element_type=jnp.float32)
            gk = jnp.concatenate(
                [gkc[r, at, :] for r in range(rank) for _ in range(rows // lanes)], axis=1)
            s = (s * coef + gq) - gk
            kpos = base + lax.broadcasted_iota(jnp.int32, (count, 1), 0)
            seen = kpos >= start
            if causal:
                seen = seen & (kpos <= qpos)
            s = jnp.where(seen, s, jnp.float32(-1e30))
            m_new = jnp.maximum(m, jnp.max(s, axis=0, keepdims=True))
            prob = jnp.exp2(s - m_new)
            shrink = jnp.exp2(m - m_new)
            l = l * shrink + jnp.sum(prob, axis=0, keepdims=True)
            acc = acc * shrink + lax.dot_general(
                vall[at], prob.astype(jnp.bfloat16), (((0,), (0,)), ((), ())),
                preferred_element_type=jnp.float32)
            return m_new, l, acc

        wide = 2 * rows
        state = (jnp.full((1, rank * rows), -1e20, jnp.float32),
                 jnp.zeros((1, rank * rows), jnp.float32),
                 jnp.zeros((HD, rank * rows), jnp.float32))
        state = lax.fori_loop(0, 2 * zq, lambda i, s: attend(i * wide, wide, False, s), state)
        m, l, acc = lax.fori_loop(
            0, p + 1, lambda i, s: attend((zq * PLANE + i) * rows, rows, True, s), state)
        res = acc / l
        for r in range(rank):
            att[zq, :, r * HD:(r + 1) * HD] = jnp.transpose(
                res[:, r * rows:(r + 1) * rows]).astype(jnp.bfloat16)

        @pl.when(zq != z)
        def _():
            remote(att.at[zq], arr.at[z], a_send.at[zq], a_recv.at[z], there(zq)).start()

    def forwards(a):
        @pl.loop(0, GROUP - 1)
        def _(i):
            forward(a, ascending(i))

    z_sends(UP)
    forwards(GATE)
    spread_own(DOWN)
    for load in loads:
        load.wait()
    own = pltpu.make_async_copy(att.at[z], arr.at[z], own_sem.at[0])
    own.start()
    own.wait()
    for d in range(1, GROUP):
        zs = (z + d) % GROUP
        at = arr.at[zs]
        remote(at, at, a_send.at[zs], a_recv.at[zs], mate).wait_recv()
    tile = 512

    @pl.loop(0, d_model // tile)
    def _(j):
        at = span(j, tile)
        total = jnp.dot(arr[0], ow_ref[0:qcols, at], preferred_element_type=jnp.float32)
        for g in range(1, GROUP):
            total += jnp.dot(arr[g], ow_ref[g * qcols:(g + 1) * qcols, at],
                             preferred_element_type=jnp.float32)
        pbuf[0, :, at] = total[:half].astype(jnp.bfloat16)
        pbuf[1, :, at] = total[half:].astype(jnp.bfloat16)

    swap = remote(pbuf.at[other], pgot, t_send, t_recv, mate)
    swap.start()
    swap.wait()
    projected = pbuf[core].astype(jnp.float32) + pgot[...].astype(jnp.float32)
    power = jnp.mean(projected * projected, axis=-1, keepdims=True)
    middle = resid_ref[...].astype(jnp.float32) + ag_ref[...] * projected * lax.rsqrt(power + 1e-06)
    mid[...] = middle
    mpower = jnp.mean(middle * middle, axis=-1, keepdims=True)
    nall[z, core] = (mg_ref[...] * middle * lax.rsqrt(mpower + 1e-06)).astype(jnp.bfloat16)

    def relay(zb, side, send_sem):
        block = nall.at[zb, core]
        return remote(block, block, send_sem, n_recv.at[zb],
                      ((z + 1 - 2 * side) * PLANE + p, core))

    def share(zb):
        block = nall.at[zb, core]
        return remote(block, block, f_send.at[zb], f_recv.at[zb], mate)

    def onward(side):
        return (side == 0) & (z < GROUP - 1) | (side == 1) & (z > 0)

    for side in (0, 1):
        @pl.when(onward(side))
        def _():
            relay(z, side, o_send.at[side]).start()
    share(z).start()

    def arrive(d):
        for side in (0, 1):
            zb = z - d if side == 0 else z + d

            @pl.when((zb >= 0) & (zb < GROUP))
            def _():
                block = nall.at[zb, core]
                remote(block, block, n_send.at[zb], n_recv.at[zb], mate).wait_recv()
                @pl.when(onward(side))
                def _():
                    relay(zb, side, n_send.at[zb]).start()
                share(zb).start()

    mate_z = z + 1 - 2 * (z % 2)
    far = GROUP // 2 - (z // 2) * 2
    at_end = (z == 0) | (z == GROUP - 1)

    def expand(zb):
        over = nall.at[zb, other]
        remote(over, over, f_send.at[zb], f_recv.at[zb], mate).wait_recv()
        rows_in = jnp.concatenate([nall[zb, 0], nall[zb, 1]], axis=0)
        ftile = 256
        for j in range(fcols // ftile):
            at = slice(j * ftile, (j + 1) * ftile)
            gate = jnp.dot(rows_in, gw[:, at], preferred_element_type=jnp.float32)
            up = jnp.dot(rows_in, uw[:, at], preferred_element_type=jnp.float32)
            hid[zb, :, at] = (gate / (1.0 + jnp.exp(-gate)) * up).astype(jnp.bfloat16)

    gcols = PLANE * wcols

    def trade(zb, g):
        at = span(g, gcols)
        return remote(part.at[zb, other, :, at], pair.at[zb, :, at], x_send.at[zb, g],
                      x_recv.at[zb, g], mate)

    def lower(zb, g):
        at = span(g, gcols)
        total = jnp.dot(hid[zb], dw[:, at], preferred_element_type=jnp.float32)
        part[zb, 0, :, at] = total[:half].astype(jnp.bfloat16)
        part[zb, 1, :, at] = total[half:].astype(jnp.bfloat16)
        trade(zb, g).start()

    def both(zb, at):
        return part[zb, core, :, at].astype(jnp.float32) + pair[zb, :, at].astype(jnp.float32)

    def give(zb, g):
        at = span(g, gcols)
        return remote(red.at[zb, :, at], got.at[0, :, at], r_send.at[zb, g], r_recv.at[0, g],
                      there(zb))

    def give_far(zb, g):
        at = span(g, gcols)
        return remote(red.at[zb, :, at], got.at[1, :, at], r_send.at[zb, g], r_recv.at[1, g],
                      there(zb))

    def give_comb(j, g):
        at = span(g, gcols)
        return remote(red.at[far + j, :, at], comb.at[j, :, at], r_send.at[far + j, g],
                      c_recv.at[j, g], there(mate_z))

    forwards(UP)
    arrive(1)
    z_sends(DOWN)
    arrive(2)

    @pl.loop(0, GROUP)
    def _(zs):
        for a in (GATE, UP):
            for e in neighbours:
                p_arrival(a, zs, e)

    expand(z)
    expand(mate_z)
    forwards(DOWN)
    arrive(3)

    @pl.loop(0, GROUP)
    def _(g):
        at = span(g, gcols)
        for e in neighbours:
            p_arrival(DOWN, g, e)
        lower(mate_z, g)
        lower(z, g)
        trade(mate_z, g).wait()
        red[mate_z, :, at] = both(mate_z, at).astype(jnp.bfloat16)
        give(mate_z, g).start()
        trade(z, g).wait()

    @pl.loop(0, 2)
    def _(j):
        expand(far + j)

    @pl.loop(0, GROUP + 1)
    def _(s):
        @pl.when(s < GROUP)
        def _():
            at = span(s, gcols)
            for j in (0, 1):
                lower(far + j, s)
            for j in (0, 1):
                trade(far + j, s).wait()

                @pl.when(at_end)
                def _():
                    red[far + j, :, at] = both(far + j, at).astype(jnp.bfloat16)
                    give_comb(j, s).start()

        @pl.when((s > 0) & (z > 0) & (z < GROUP - 1))
        def _():
            g = s - 1
            at = span(g, gcols)
            for j in (0, 1):
                give_comb(j, g).wait_recv()
                red[far + j, :, at] = (both(far + j, at)
                                       + comb[j, :, at].astype(jnp.float32)).astype(jnp.bfloat16)
                give_far(far + j, g).start()

    @pl.loop(0, GROUP)
    def _(g):
        at = span(g, gcols)
        give(mate_z, g).wait_recv()
        give_far(far, g).wait_recv()
        total = both(z, at) + got[0, :, at].astype(jnp.float32) + got[1, :, at].astype(jnp.float32)
        out_ref[:, at] = (mid[:, at] + 0.5 * total).astype(jnp.bfloat16)

    for d in range(1, GROUP):
        zb = (z + d) % GROUP
        for a in range(7):
            z_copy(a, zb).wait_send()
        remote(att.at[zb], arr.at[z], a_send.at[zb], a_recv.at[z], there(zb)).wait_send()

        @pl.loop(0, GROUP)
        def _(g):
            give(zb, g).wait_send()

    for a in range(6):
        for e in neighbours:
            p_own(a, e).wait_send()
            for d in range(1, GROUP):
                p_copy(a, (z + d) % GROUP, e).wait_send()
    share(z).wait_send()
    for side in (0, 1):
        @pl.when(onward(side))
        def _():
            relay(z, side, o_send.at[side]).wait_send()
    for d in range(1, GROUP):
        share((z + d) % GROUP).wait_send()
        for side in (0, 1):
            zb = z - d if side == 0 else z + d

            @pl.when((zb >= 0) & (zb < GROUP) & onward(side))
            def _():
                relay(zb, side, n_send.at[zb]).wait_send()


def grouped(
    sp, resid, queries, keys, values, log_gates, documents, out_weight, attn_gain, mlp_gain,
    gate_weight, up_weight, down_weight,
):
    rows, ff = keys.shape[0], gate_weight.shape[1] // GROUP
    half, d_model = resid.shape
    tokens = rows * sp
    qcols = queries.shape[1] // GROUP
    rank = qcols // HD
    bf, f32 = jnp.bfloat16, jnp.float32
    dma = pltpu.SemaphoreType.DMA
    return pl.pallas_call(
        layer_kernel,
        out_shape=jax.ShapeDtypeStruct(resid.shape, bf),
        in_specs=[VMEM] * 5 + [ANY] * 2 + [VMEM] * 2 + [ANY] * 3,
        out_specs=VMEM,
        scratch_shapes=[
            pltpu.VMEM(out_weight.shape, bf),
            pltpu.VMEM(resid.shape, bf),
            pltpu.VMEM((tokens, HD), bf),
            pltpu.VMEM((tokens, HD), bf),
            pltpu.VMEM((sp, 1, rows), jnp.int32),
            pltpu.VMEM((GROUP, rows, qcols), bf),
            pltpu.VMEM((rank, tokens, 128), f32),
            pltpu.VMEM((d_model, ff), bf),
            pltpu.VMEM((d_model, ff), bf),
            pltpu.VMEM((ff, d_model), bf),
            pltpu.VMEM((GROUP, rows, qcols), bf),
            pltpu.VMEM((GROUP, rows, qcols), bf),
            pltpu.VMEM((2, half, d_model), bf),
            pltpu.VMEM((half, d_model), bf),
            pltpu.VMEM((half, d_model), f32),
            pltpu.VMEM((GROUP, 2, half, d_model), bf),
            pltpu.VMEM((GROUP, rows, ff), bf),
            pltpu.VMEM((GROUP, 2, half, d_model), bf),
            pltpu.VMEM((GROUP, half, d_model), bf),
            pltpu.VMEM((GROUP, half, d_model), bf),
            pltpu.VMEM((2, half, d_model), bf),
            pltpu.VMEM((2, half, d_model), bf),
            dma((7, GROUP)), dma((7, GROUP)), dma((6, GROUP, 3)), dma((6, GROUP, 3)), dma((7,)),
            dma((2,)),
            dma((GROUP,)), dma((GROUP,)), dma, dma,
            dma((2,)), dma((GROUP,)), dma((GROUP,)), dma((GROUP,)), dma((GROUP,)),
            dma((GROUP, GROUP)), dma((GROUP, GROUP)), dma((GROUP, GROUP)), dma((2, GROUP)),
            dma((2, GROUP)),
        ],
        compiler_params=pltpu.CompilerParams(
            collective_id=0, has_side_effects=True, vmem_limit_bytes=62 * 1024 * 1024),
    )(queries, keys, values, documents[None, :], log_gates,
      out_weight, resid, attn_gain[None, :], mlp_gain[None, :], gate_weight, up_weight,
      down_weight)


def solution(mesh):
    placed = (
        P(("sp", "tp"), None),
        P("sp", "tp"),
        P("sp", "tp"),
        P("sp", "tp"),
        P("tp", None),
        P("sp"),
        P("tp", None),
        P(),
        P(),
        P("sp", "tp"),
        P("sp", "tp"),
        P("tp", "sp"),
    )
    sp, tp = mesh.shape["sp"], mesh.shape["tp"]

    def layer(*args):
        kv_dev = args[2].shape[1] // HD
        fits = tp == 2 and sp == GROUP * PLANE and kv_dev == GROUP
        return grouped(sp, *args) if fits else local(*args)

    return jax.shard_map(
        layer, mesh=mesh, in_specs=placed, out_specs=P(("sp", "tp"), None), check_vma=False
    )
```

```python
import math

import jax
import jax.numpy as jnp
from jax import lax
from jax.experimental import pallas as pl
from jax.experimental.pallas import tpu as pltpu
from jax.sharding import PartitionSpec as P

HD = 128


def local(
    resid,
    queries,
    keys,
    values,
    log_gates,
    documents,
    out_weight,
    attn_gain,
    mlp_gain,
    gate_weight,
    up_weight,
    down_weight,
):
    tok_rows = queries.shape[0]
    kv_dev = keys.shape[1] // HD
    heads_dev = log_gates.shape[0]
    group_size = heads_dev // kv_dev
    score_scale = 1.0 / math.sqrt(HD)
    own_start = lax.axis_index("sp") * tok_rows
    own_last = own_start + tok_rows - 1
    first_doc = documents[0]
    query_pos = own_start + lax.iota(jnp.int32, tok_rows)
    query_heads = queries.reshape(tok_rows, kv_dev, group_size, HD)
    key_gates_all = log_gates.reshape(kv_dev, group_size, log_gates.shape[1])
    query_gates = lax.dynamic_slice_in_dim(key_gates_all, own_start, tok_rows, 2)
    collected = (
        lax.all_gather(gate_weight, "sp", axis=0, tiled=True),
        lax.all_gather(up_weight, "sp", axis=0, tiled=True),
        lax.all_gather(down_weight, "sp", axis=1, tiled=True),
    )
    residual_rows = resid.astype(jnp.float32)

    def attend_block(running, key_rows, value_rows, doc_rows, first_row):
        run_max, run_sum, accumulated = running
        key_count = key_rows.shape[0]
        scores = (
            jnp.einsum(
                "tkgd,skd->kgts",
                query_heads,
                key_rows.reshape(key_count, kv_dev, HD),
                preferred_element_type=jnp.float32,
            )
            * score_scale
        )
        key_gates = lax.dynamic_slice_in_dim(key_gates_all, first_row, key_count, 2)
        scores = scores + query_gates[..., None] - key_gates[:, :, None, :]
        key_pos = first_row + lax.iota(jnp.int32, key_count)
        visible = (key_pos[None, :] <= query_pos[:, None]) & (
            doc_rows[None, :] == documents[:, None]
        )
        scores = jnp.where(visible, scores, jnp.float32(-1e30))
        new_max = jnp.maximum(run_max, jnp.max(scores, axis=-1))
        probs = jnp.where(visible, jnp.exp(scores - new_max[..., None]), jnp.float32(0.0))
        shrink = jnp.exp(run_max - new_max)
        run_sum = run_sum * shrink + jnp.sum(probs, axis=-1)
        weighted = jnp.einsum(
            "kgts,skd->kgtd",
            probs.astype(jnp.bfloat16),
            value_rows.reshape(key_count, kv_dev, HD),
            preferred_element_type=jnp.float32,
        )
        accumulated = accumulated * shrink[..., None] + weighted
        return (new_max, run_sum, accumulated)

    def maybe_attend(running, key_rows, value_rows, doc_rows, first_row):
        needed = (first_row <= own_last) & (doc_rows[-1] >= first_doc)

        def compute(state):
            return attend_block(state, key_rows, value_rows, doc_rows, first_row)

        def keep(state):
            return state

        return lax.cond(needed, compute, keep, running)

    start_state = (
        jnp.full((kv_dev, group_size, tok_rows), -1e30, jnp.float32),
        jnp.zeros((kv_dev, group_size, tok_rows), jnp.float32),
        jnp.zeros((kv_dev, group_size, tok_rows, HD), jnp.float32),
    )
    key_rows = lax.all_gather(keys, "sp", axis=0, tiled=True)
    value_rows = lax.all_gather(values, "sp", axis=0, tiled=True)
    doc_rows = lax.all_gather(documents, "sp", axis=0, tiled=True)
    key_count = key_rows.shape[0]
    block_len = math.gcd(key_count, 1024)

    def advance(block_index, inner):
        offset = block_index * block_len
        return maybe_attend(
            inner,
            lax.dynamic_slice_in_dim(key_rows, offset, block_len, 0),
            lax.dynamic_slice_in_dim(value_rows, offset, block_len, 0),
            lax.dynamic_slice_in_dim(doc_rows, offset, block_len, 0),
            offset,
        )

    run_max, run_sum, accumulated = lax.fori_loop(0, key_count // block_len, advance, start_state)
    attended = accumulated / run_sum[..., None]
    attended = (
        jnp.transpose(attended, (2, 0, 1, 3)).reshape(tok_rows, heads_dev * HD).astype(jnp.bfloat16)
    )
    rows_slice = attended
    projected = lax.psum_scatter(
        jnp.dot(rows_slice, out_weight, preferred_element_type=jnp.float32).astype(jnp.bfloat16),
        "tp",
        scatter_dimension=0,
        tiled=True,
    ).astype(jnp.float32)
    power = jnp.mean(projected * projected, axis=-1, keepdims=True)
    middle = residual_rows + attn_gain * projected * lax.rsqrt(power + 1e-06)
    middle_power = jnp.mean(middle * middle, axis=-1, keepdims=True)
    normed = (mlp_gain * middle * lax.rsqrt(middle_power + 1e-06)).astype(jnp.bfloat16)
    normed_all = lax.all_gather(normed, "tp", axis=0, tiled=True)
    gate_full, up_full, down_full = collected
    gate_act = jnp.dot(normed_all, gate_full, preferred_element_type=jnp.float32)
    up_act = jnp.dot(normed_all, up_full, preferred_element_type=jnp.float32)
    hidden = (jax.nn.silu(gate_act) * up_act).astype(jnp.bfloat16)
    rows_slice = hidden
    lowered = lax.psum_scatter(
        jnp.dot(rows_slice, down_full, preferred_element_type=jnp.float32).astype(jnp.bfloat16),
        "tp",
        scatter_dimension=0,
        tiled=True,
    ).astype(jnp.float32)
    return (middle + 0.5 * lowered).astype(jnp.bfloat16)


GROUP = 4
PLANE = 4
MESH = pl.DeviceIdType.MESH
LOG2E = 1.4426950408889634
VMEM = pl.BlockSpec(memory_space=pltpu.VMEM)
ANY = pl.BlockSpec(memory_space=pl.ANY)
K, V, DOC, GATE, UP, DOWN, Q = range(7)


def remote(src, dst, send_sem, recv_sem, target):
    return pltpu.make_async_remote_copy(
        src_ref=src,
        dst_ref=dst,
        send_sem=send_sem,
        recv_sem=recv_sem,
        device_id=target,
        device_id_type=MESH,
    )


def span(index, width):
    return pl.ds(pl.multiple_of(index * width, width), width)


def layer_kernel(
    q_ref, k_ref, v_ref, d_ref, lg_ref, ow_hbm, resid_hbm, ag_ref, mg_ref, g_ref, u_ref, w_ref,
    out_ref,
    ow_ref, resid_ref,
    kall, vall, docs, qs, gkc, gw, uw, dw, att, arr, pbuf, pgot, mid, nall, hid, part, pair, red,
    got, comb,
    z_send, z_recv, p_send, p_recv, own_sem, load_sem, a_send, a_recv, t_send, t_recv,
    o_send, n_send, n_recv, f_send, f_recv, x_send, x_recv, r_send, r_recv, c_recv,
):
    me = lax.axis_index("sp")
    core = lax.axis_index("tp")
    z, p = me // PLANE, me % PLANE
    px, py = p % 2, p // 2
    other = 1 - core
    mate = (me, other)
    rows = k_ref.shape[0]
    qcols = q_ref.shape[1] // GROUP
    rank = qcols // HD
    fcols = g_ref.shape[1] // GROUP
    wrows, wcols = g_ref.shape[0], w_ref.shape[1]
    half, d_model = resid_hbm.shape
    coef = LOG2E / math.sqrt(HD)
    neighbours = (1, 2, 3)

    def peer(e):
        x = px if e == 2 else 1 - px
        y = py if e == 1 else 1 - py
        return y * 2 + x

    def near(e):
        return (z * PLANE + peer(e), core)

    def there(zb):
        return (zb * PLANE + p, core)

    def place(a, k):
        if a == K:
            return kall.at[span(k, rows)]
        if a == V:
            return vall.at[span(k, rows)]
        if a == DOC:
            return docs.at[k]
        if a == GATE:
            return gw.at[span(k, wrows)]
        if a == UP:
            return uw.at[span(k, wrows)]
        if a == DOWN:
            return dw.at[:, span(k, wcols)]
        return qs.at[k // PLANE]

    def piece(a, to):
        if a == K:
            return k_ref.at[:, span(to, HD)]
        if a == V:
            return v_ref.at[:, span(to, HD)]
        if a == DOC:
            return d_ref.at[...]
        if a == GATE:
            return g_ref.at[:, span(to, fcols)]
        if a == UP:
            return u_ref.at[:, span(to, fcols)]
        if a == DOWN:
            return w_ref.at[span(to, fcols)]
        return q_ref.at[:, span(to, qcols)]

    barrier = pltpu.get_barrier_semaphore()
    for d in range(1, GROUP):
        pl.semaphore_signal(barrier, inc=1, device_id=there((z + d) % GROUP), device_id_type=MESH)
    loads = (pltpu.make_async_copy(ow_hbm, ow_ref, load_sem.at[0]),
             pltpu.make_async_copy(resid_hbm, resid_ref, load_sem.at[1]))
    for e in neighbours:
        pl.semaphore_signal(barrier, inc=1, device_id=near(e), device_id_type=MESH)
    pl.semaphore_signal(barrier, inc=1, device_id=mate, device_id_type=MESH)
    pl.semaphore_wait(barrier, 7)

    def z_copy(a, to):
        return remote(piece(a, to), place(a, me), z_send.at[a, to], z_recv.at[a, z], there(to))

    def z_sends(a):
        for d in (1, 3, 2):
            z_copy(a, (z + d) % GROUP).start()

    def z_arrival(a, zs):
        at = place(a, zs * PLANE + p)
        remote(at, at, z_send.at[a, z], z_recv.at[a, zs], mate).wait_recv()

    def own_copy(a):
        return pltpu.make_async_copy(piece(a, z), place(a, me), own_sem.at[a])

    def p_copy(a, zs, e):
        at = place(a, zs * PLANE + p)
        return remote(at, at, p_send.at[a, zs, e - 1], p_recv.at[a, zs, e - 1], near(e))

    def p_own(a, e):
        return remote(piece(a, z), place(a, me), p_send.at[a, z, e - 1], p_recv.at[a, z, e - 1],
                      near(e))

    def p_arrival(a, zs, e):
        at = place(a, zs * PLANE + peer(e))
        remote(at, at, p_send.at[a, zs, e - 1], p_recv.at[a, zs, e - 1], mate).wait_recv()

    def spread_own(a):
        for e in neighbours:
            p_own(a, e).start()

    def forward(a, zs):
        z_arrival(a, zs)
        for e in neighbours:
            p_copy(a, zs, e).start()

    for a in (DOC, K, V, Q, GATE):
        z_sends(a)
    for a in (DOC, K, V):
        spread_own(a)
    for a in range(7):
        own_copy(a).start()
    for load in loads:
        load.start()

    lanes = 128

    def gate_row(r, at):
        block = lg_ref[:, at]
        chosen = lax.broadcasted_iota(jnp.int32, block.shape, 0) == z * rank + r
        return jnp.sum(jnp.where(chosen, block, 0.0), axis=0, keepdims=True) * LOG2E

    @pl.loop(0, kall.shape[0] // lanes)
    def _(j):
        at = span(j, lanes)
        for r in range(rank):
            row = gate_row(r, at)
            gkc[r, at, :] = jnp.transpose(jnp.broadcast_to(row, (lanes, lanes)))

    def ascending(i):
        return i + (i - z + GROUP) // GROUP

    def forwards(a):
        @pl.loop(0, GROUP - 1)
        def _(i):
            forward(a, ascending(i))

    forwards(DOC)

    @pl.loop(0, GROUP - 2)
    def _(i):
        forward(K, ascending(i))
        forward(V, ascending(i))

    for a in range(7):
        own_copy(a).wait()

    @pl.loop(0, GROUP)
    def _(zs):
        for e in neighbours:
            p_arrival(DOC, zs, e)

    every_doc = docs[...]

    def below(level):
        total = jnp.sum((every_doc < level).astype(jnp.float32), axis=0)
        return jnp.sum(total, axis=1, keepdims=True)

    first_of_1, first_of_2 = below(1), below(2)

    @pl.loop(0, GROUP)
    def _(zq):
        @pl.when(zq == 1)
        def _():
            forward(K, ascending(GROUP - 2))
            forward(V, ascending(GROUP - 2))
            spread_own(GATE)
            spread_own(UP)
            z_sends(UP)

        @pl.when(zq == GROUP - 1)
        def _():
            forwards(GATE)

        @pl.when(zq != z)
        def _():
            z_arrival(Q, zq)

        for e in neighbours:
            p_arrival(K, zq, e)
            p_arrival(V, zq, e)
        block = zq * PLANE + p
        q = jnp.concatenate([qs[zq, :, r * HD:(r + 1) * HD] for r in range(rank)], axis=0)
        own = span(block, rows)
        gq = jnp.concatenate([gate_row(r, own) for r in range(rank)], axis=1)
        dq = docs[block]
        start = jnp.where(dq == 0, 0.0, jnp.where(dq == 1, first_of_1, first_of_2))
        start = jnp.concatenate([start.astype(jnp.int32)] * rank, axis=1)
        qpos = block * rows + lax.broadcasted_iota(jnp.int32, (1, rows), 1)
        qpos = jnp.concatenate([qpos] * rank, axis=1)

        def attend(base, count, causal, state):
            m, l, acc = state
            at = pl.ds(pl.multiple_of(base, count), count)
            s = lax.dot_general(kall[at], q, (((1,), (1,)), ((), ())),
                                preferred_element_type=jnp.float32)
            gk = jnp.concatenate(
                [gkc[r, at, :] for r in range(rank) for _ in range(rows // lanes)], axis=1)
            s = (s * coef + gq) - gk
            kpos = base + lax.broadcasted_iota(jnp.int32, (count, 1), 0)
            seen = kpos >= start
            if causal:
                seen = seen & (kpos <= qpos)
            s = jnp.where(seen, s, jnp.float32(-1e30))
            m_new = jnp.maximum(m, jnp.max(s, axis=0, keepdims=True))
            prob = jnp.exp2(s - m_new)
            shrink = jnp.exp2(m - m_new)
            l = l * shrink + jnp.sum(prob, axis=0, keepdims=True)
            acc = acc * shrink + lax.dot_general(
                vall[at], prob.astype(jnp.bfloat16), (((0,), (0,)), ((), ())),
                preferred_element_type=jnp.float32)
            return m_new, l, acc

        wide = 2 * rows
        state = (jnp.full((1, rank * rows), -1e20, jnp.float32),
                 jnp.zeros((1, rank * rows), jnp.float32),
                 jnp.zeros((HD, rank * rows), jnp.float32))
        state = lax.fori_loop(0, 2 * zq, lambda i, s: attend(i * wide, wide, False, s), state)
        m, l, acc = lax.fori_loop(
            0, p + 1, lambda i, s: attend((zq * PLANE + i) * rows, rows, True, s), state)
        res = acc / l
        for r in range(rank):
            att[zq, :, r * HD:(r + 1) * HD] = jnp.transpose(
                res[:, r * rows:(r + 1) * rows]).astype(jnp.bfloat16)

        @pl.when(zq != z)
        def _():
            remote(att.at[zq], arr.at[z], a_send.at[zq], a_recv.at[z], there(zq)).start()

    z_sends(DOWN)
    forwards(UP)
    spread_own(DOWN)
    for load in loads:
        load.wait()
    own = pltpu.make_async_copy(att.at[z], arr.at[z], own_sem.at[0])
    own.start()
    own.wait()
    for d in range(1, GROUP):
        zs = (z + d) % GROUP
        at = arr.at[zs]
        remote(at, at, a_send.at[zs], a_recv.at[zs], mate).wait_recv()
    tile = 512

    @pl.loop(0, d_model // tile)
    def _(j):
        at = span(j, tile)
        total = jnp.dot(arr[0], ow_ref[0:qcols, at], preferred_element_type=jnp.float32)
        for g in range(1, GROUP):
            total += jnp.dot(arr[g], ow_ref[g * qcols:(g + 1) * qcols, at],
                             preferred_element_type=jnp.float32)
        pbuf[0, :, at] = total[:half].astype(jnp.bfloat16)
        pbuf[1, :, at] = total[half:].astype(jnp.bfloat16)

    swap = remote(pbuf.at[other], pgot, t_send, t_recv, mate)
    swap.start()
    swap.wait()
    projected = pbuf[core].astype(jnp.float32) + pgot[...].astype(jnp.float32)
    power = jnp.mean(projected * projected, axis=-1, keepdims=True)
    middle = resid_ref[...].astype(jnp.float32) + ag_ref[...] * projected * lax.rsqrt(power + 1e-06)
    mid[...] = middle
    mpower = jnp.mean(middle * middle, axis=-1, keepdims=True)
    nall[z, core] = (mg_ref[...] * middle * lax.rsqrt(mpower + 1e-06)).astype(jnp.bfloat16)

    piece_rows = half // 2

    def relay(zb, side, c, send_sem):
        block = nall.at[zb, core, span(c, piece_rows)]
        return remote(block, block, send_sem, n_recv.at[zb, c],
                      ((z + 1 - 2 * side) * PLANE + p, core))

    def share(zb, c):
        block = nall.at[zb, core, span(c, piece_rows)]
        return remote(block, block, f_send.at[zb, c], f_recv.at[zb, c], mate)

    def shared(zb, c):
        over = nall.at[zb, other, span(c, piece_rows)]
        remote(over, over, f_send.at[zb, c], f_recv.at[zb, c], mate).wait_recv()

    def onward(side):
        return (side == 0) & (z < GROUP - 1) | (side == 1) & (z > 0)

    for c in (0, 1):
        for side in (0, 1):
            @pl.when(onward(side))
            def _():
                relay(z, side, c, o_send.at[side, c]).start()
    for c in (0, 1):
        share(z, c).start()

    def arrive(d, c):
        for side in (0, 1):
            zb = z - d if side == 0 else z + d

            @pl.when((zb >= 0) & (zb < GROUP))
            def _():
                block = nall.at[zb, core, span(c, piece_rows)]
                remote(block, block, n_send.at[zb, c], n_recv.at[zb, c], mate).wait_recv()
                @pl.when(onward(side))
                def _():
                    relay(zb, side, c, n_send.at[zb, c]).start()
                share(zb, c).start()

    mate_z = z + 1 - 2 * (z % 2)
    far = GROUP // 2 - (z // 2) * 2
    at_end = (z == 0) | (z == GROUP - 1)

    def expand(zb, c):
        shared(zb, c)
        rows_in = jnp.concatenate(
            [nall[zb, i, span(c, piece_rows), :] for i in (0, 1)], axis=0)
        ftile = 256
        for j in range(fcols // ftile):
            at = slice(j * ftile, (j + 1) * ftile)
            gate = jnp.dot(rows_in, gw[:, at], preferred_element_type=jnp.float32)
            up = jnp.dot(rows_in, uw[:, at], preferred_element_type=jnp.float32)
            hid[zb, c, :, at] = (gate / (1.0 + jnp.exp(-gate)) * up).astype(jnp.bfloat16)

    gcols = PLANE * wcols
    hcols = d_model // 2

    def trade(zb, g):
        at = span(g, gcols)
        return remote(part.at[zb, other, :, at], pair.at[zb, :, at], x_send.at[zb, g],
                      x_recv.at[zb, g], mate)

    def lower(zb, g):
        at = span(g, gcols)
        rows_in = jnp.concatenate([hid[zb, 0], hid[zb, 1]], axis=0)
        total = jnp.dot(rows_in, dw[:, at], preferred_element_type=jnp.float32)
        for c in (0, 1):
            for i in (0, 1):
                first = (2 * c + i) * piece_rows
                part[zb, i, c * piece_rows:(c + 1) * piece_rows, at] = (
                    total[first:first + piece_rows].astype(jnp.bfloat16))
        trade(zb, g).start()

    def both(zb, at):
        return part[zb, core, :, at].astype(jnp.float32) + pair[zb, :, at].astype(jnp.float32)

    def give(zb, g):
        at = span(g, gcols)
        return remote(red.at[zb, :, at], got.at[0, :, at], r_send.at[zb, g], r_recv.at[0, g],
                      there(zb))

    def corner(c, h):
        return span(c, piece_rows), slice(h * hcols, (h + 1) * hcols)

    def trade_far(zb, c, h):
        rs, cs = corner(c, h)
        return remote(part.at[zb, other, rs, cs], pair.at[zb, rs, cs], x_send.at[zb, 2 * c + h],
                      x_recv.at[zb, 2 * c + h], mate)

    def give_far(zb, c, h):
        rs, cs = corner(c, h)
        return remote(red.at[zb, rs, cs], got.at[1, rs, cs], r_send.at[zb, 2 * c + h],
                      r_recv.at[1, 2 * c + h], there(zb))

    def give_comb(t, zb, c, h):
        rs, cs = corner(c, h)
        return remote(red.at[zb, rs, cs], comb.at[t, rs, cs], r_send.at[zb, 2 * c + h],
                      c_recv.at[t, 2 * c + h], there(mate_z))

    def both_far(zb, rs, cs):
        return part[zb, core, rs, cs].astype(jnp.float32) + pair[zb, rs, cs].astype(jnp.float32)

    forwards(DOWN)
    arrive(1, 0)
    arrive(1, 1)

    @pl.loop(0, GROUP)
    def _(zs):
        for a in (GATE, UP):
            for e in neighbours:
                p_arrival(a, zs, e)

    @pl.loop(0, 2)
    def _(c):
        expand(z, c)
        arrive(2, c)

    @pl.loop(0, 2)
    def _(c):
        expand(mate_z, c)

    @pl.loop(0, GROUP)
    def _(g):
        at = span(g, gcols)
        for e in neighbours:
            p_arrival(DOWN, g, e)
        lower(mate_z, g)
        lower(z, g)
        trade(mate_z, g).wait()
        red[mate_z, :, at] = both(mate_z, at).astype(jnp.bfloat16)
        give(mate_z, g).start()
        trade(z, g).wait()

    def send_far(t):
        zb = far + t + (1 - 2 * t) * (z // 2)

        @pl.loop(0, 2)
        def _(c):
            if t == 1:
                arrive(3, c)
            expand(zb, c)
            for h in (0, 1):
                rs, cs = corner(c, h)
                total = jnp.dot(hid[zb, c], dw[:, cs], preferred_element_type=jnp.float32)
                for i in (0, 1):
                    part[zb, i, rs, cs] = total[i * piece_rows:(i + 1) * piece_rows].astype(
                        jnp.bfloat16)
                trade_far(zb, c, h).start()
            for h in (0, 1):
                rs, cs = corner(c, h)
                trade_far(zb, c, h).wait()

                @pl.when(at_end)
                def _():
                    red[zb, rs, cs] = both_far(zb, rs, cs).astype(jnp.bfloat16)
                    give_comb(t, zb, c, h).start()

        @pl.when((z > 0) & (z < GROUP - 1))
        def _():
            @pl.loop(0, 2)
            def _(c):
                for h in (0, 1):
                    rs, cs = corner(c, h)
                    give_comb(t, zb, c, h).wait_recv()
                    red[zb, rs, cs] = (both_far(zb, rs, cs)
                                       + comb[t, rs, cs].astype(jnp.float32)).astype(jnp.bfloat16)
                    give_far(zb, c, h).start()

    send_far(0)
    send_far(1)

    for c in (0, 1):
        for h in (0, 1):
            give_far(far, c, h).wait_recv()

    @pl.loop(0, GROUP)
    def _(g):
        at = span(g, gcols)
        give(mate_z, g).wait_recv()
        total = both(z, at) + got[0, :, at].astype(jnp.float32) + got[1, :, at].astype(jnp.float32)
        out_ref[:, at] = (mid[:, at] + 0.5 * total).astype(jnp.bfloat16)

    for d in range(1, GROUP):
        zb = (z + d) % GROUP
        for a in range(7):
            z_copy(a, zb).wait_send()
        remote(att.at[zb], arr.at[z], a_send.at[zb], a_recv.at[z], there(zb)).wait_send()

        @pl.loop(0, GROUP)
        def _(g):
            give(zb, g).wait_send()

    for a in range(6):
        for e in neighbours:
            p_own(a, e).wait_send()
            for d in range(1, GROUP):
                p_copy(a, (z + d) % GROUP, e).wait_send()
    for c in (0, 1):
        share(z, c).wait_send()
        for side in (0, 1):
            @pl.when(onward(side))
            def _():
                relay(z, side, c, o_send.at[side, c]).wait_send()
        for d in range(1, GROUP):
            share((z + d) % GROUP, c).wait_send()
            for side in (0, 1):
                zb = z - d if side == 0 else z + d

                @pl.when((zb >= 0) & (zb < GROUP) & onward(side))
                def _():
                    relay(zb, side, c, n_send.at[zb, c]).wait_send()


def grouped(
    sp, resid, queries, keys, values, log_gates, documents, out_weight, attn_gain, mlp_gain,
    gate_weight, up_weight, down_weight,
):
    rows, ff = keys.shape[0], gate_weight.shape[1] // GROUP
    half, d_model = resid.shape
    tokens = rows * sp
    qcols = queries.shape[1] // GROUP
    rank = qcols // HD
    bf, f32 = jnp.bfloat16, jnp.float32
    dma = pltpu.SemaphoreType.DMA
    return pl.pallas_call(
        layer_kernel,
        out_shape=jax.ShapeDtypeStruct(resid.shape, bf),
        in_specs=[VMEM] * 5 + [ANY] * 2 + [VMEM] * 2 + [ANY] * 3,
        out_specs=VMEM,
        scratch_shapes=[
            pltpu.VMEM(out_weight.shape, bf),
            pltpu.VMEM(resid.shape, bf),
            pltpu.VMEM((tokens, HD), bf),
            pltpu.VMEM((tokens, HD), bf),
            pltpu.VMEM((sp, 1, rows), jnp.int32),
            pltpu.VMEM((GROUP, rows, qcols), bf),
            pltpu.VMEM((rank, tokens, 128), f32),
            pltpu.VMEM((d_model, ff), bf),
            pltpu.VMEM((d_model, ff), bf),
            pltpu.VMEM((ff, d_model), bf),
            pltpu.VMEM((GROUP, rows, qcols), bf),
            pltpu.VMEM((GROUP, rows, qcols), bf),
            pltpu.VMEM((2, half, d_model), bf),
            pltpu.VMEM((half, d_model), bf),
            pltpu.VMEM((half, d_model), f32),
            pltpu.VMEM((GROUP, 2, half, d_model), bf),
            pltpu.VMEM((GROUP, 2, half, ff), bf),
            pltpu.VMEM((GROUP, 2, half, d_model), bf),
            pltpu.VMEM((GROUP, half, d_model), bf),
            pltpu.VMEM((GROUP, half, d_model), bf),
            pltpu.VMEM((2, half, d_model), bf),
            pltpu.VMEM((2, half, d_model), bf),
            dma((7, GROUP)), dma((7, GROUP)), dma((6, GROUP, 3)), dma((6, GROUP, 3)), dma((7,)),
            dma((2,)),
            dma((GROUP,)), dma((GROUP,)), dma, dma,
            dma((2, 2)), dma((GROUP, 2)), dma((GROUP, 2)), dma((GROUP, 2)), dma((GROUP, 2)),
            dma((GROUP, GROUP)), dma((GROUP, GROUP)), dma((GROUP, GROUP)), dma((2, GROUP)),
            dma((2, GROUP)),
        ],
        compiler_params=pltpu.CompilerParams(
            collective_id=0, has_side_effects=True, vmem_limit_bytes=62 * 1024 * 1024),
    )(queries, keys, values, documents[None, :], log_gates,
      out_weight, resid, attn_gain[None, :], mlp_gain[None, :], gate_weight, up_weight,
      down_weight)


def solution(mesh):
    placed = (
        P(("sp", "tp"), None),
        P("sp", "tp"),
        P("sp", "tp"),
        P("sp", "tp"),
        P("tp", None),
        P("sp"),
        P("tp", None),
        P(),
        P(),
        P("sp", "tp"),
        P("sp", "tp"),
        P("tp", "sp"),
    )
    sp, tp = mesh.shape["sp"], mesh.shape["tp"]

    def layer(*args):
        kv_dev = args[2].shape[1] // HD
        fits = tp == 2 and sp == GROUP * PLANE and kv_dev == GROUP
        return grouped(sp, *args) if fits else local(*args)

    return jax.shard_map(
        layer, mesh=mesh, in_specs=placed, out_specs=P(("sp", "tp"), None), check_vma=False
    )
```

```python
import math

import jax
import jax.numpy as jnp
from jax import lax
from jax.experimental import pallas as pl
from jax.experimental.pallas import tpu as pltpu
from jax.sharding import PartitionSpec as P

HD = 128


def local(
    resid,
    queries,
    keys,
    values,
    log_gates,
    documents,
    out_weight,
    attn_gain,
    mlp_gain,
    gate_weight,
    up_weight,
    down_weight,
):
    tok_rows = queries.shape[0]
    kv_dev = keys.shape[1] // HD
    heads_dev = log_gates.shape[0]
    group_size = heads_dev // kv_dev
    score_scale = 1.0 / math.sqrt(HD)
    own_start = lax.axis_index("sp") * tok_rows
    own_last = own_start + tok_rows - 1
    first_doc = documents[0]
    query_pos = own_start + lax.iota(jnp.int32, tok_rows)
    query_heads = queries.reshape(tok_rows, kv_dev, group_size, HD)
    key_gates_all = log_gates.reshape(kv_dev, group_size, log_gates.shape[1])
    query_gates = lax.dynamic_slice_in_dim(key_gates_all, own_start, tok_rows, 2)
    collected = (
        lax.all_gather(gate_weight, "sp", axis=0, tiled=True),
        lax.all_gather(up_weight, "sp", axis=0, tiled=True),
        lax.all_gather(down_weight, "sp", axis=1, tiled=True),
    )
    residual_rows = resid.astype(jnp.float32)

    def attend_block(running, key_rows, value_rows, doc_rows, first_row):
        run_max, run_sum, accumulated = running
        key_count = key_rows.shape[0]
        scores = (
            jnp.einsum(
                "tkgd,skd->kgts",
                query_heads,
                key_rows.reshape(key_count, kv_dev, HD),
                preferred_element_type=jnp.float32,
            )
            * score_scale
        )
        key_gates = lax.dynamic_slice_in_dim(key_gates_all, first_row, key_count, 2)
        scores = scores + query_gates[..., None] - key_gates[:, :, None, :]
        key_pos = first_row + lax.iota(jnp.int32, key_count)
        visible = (key_pos[None, :] <= query_pos[:, None]) & (
            doc_rows[None, :] == documents[:, None]
        )
        scores = jnp.where(visible, scores, jnp.float32(-1e30))
        new_max = jnp.maximum(run_max, jnp.max(scores, axis=-1))
        probs = jnp.where(visible, jnp.exp(scores - new_max[..., None]), jnp.float32(0.0))
        shrink = jnp.exp(run_max - new_max)
        run_sum = run_sum * shrink + jnp.sum(probs, axis=-1)
        weighted = jnp.einsum(
            "kgts,skd->kgtd",
            probs.astype(jnp.bfloat16),
            value_rows.reshape(key_count, kv_dev, HD),
            preferred_element_type=jnp.float32,
        )
        accumulated = accumulated * shrink[..., None] + weighted
        return (new_max, run_sum, accumulated)

    def maybe_attend(running, key_rows, value_rows, doc_rows, first_row):
        needed = (first_row <= own_last) & (doc_rows[-1] >= first_doc)

        def compute(state):
            return attend_block(state, key_rows, value_rows, doc_rows, first_row)

        def keep(state):
            return state

        return lax.cond(needed, compute, keep, running)

    start_state = (
        jnp.full((kv_dev, group_size, tok_rows), -1e30, jnp.float32),
        jnp.zeros((kv_dev, group_size, tok_rows), jnp.float32),
        jnp.zeros((kv_dev, group_size, tok_rows, HD), jnp.float32),
    )
    key_rows = lax.all_gather(keys, "sp", axis=0, tiled=True)
    value_rows = lax.all_gather(values, "sp", axis=0, tiled=True)
    doc_rows = lax.all_gather(documents, "sp", axis=0, tiled=True)
    key_count = key_rows.shape[0]
    block_len = math.gcd(key_count, 1024)

    def advance(block_index, inner):
        offset = block_index * block_len
        return maybe_attend(
            inner,
            lax.dynamic_slice_in_dim(key_rows, offset, block_len, 0),
            lax.dynamic_slice_in_dim(value_rows, offset, block_len, 0),
            lax.dynamic_slice_in_dim(doc_rows, offset, block_len, 0),
            offset,
        )

    run_max, run_sum, accumulated = lax.fori_loop(0, key_count // block_len, advance, start_state)
    attended = accumulated / run_sum[..., None]
    attended = (
        jnp.transpose(attended, (2, 0, 1, 3)).reshape(tok_rows, heads_dev * HD).astype(jnp.bfloat16)
    )
    rows_slice = attended
    projected = lax.psum_scatter(
        jnp.dot(rows_slice, out_weight, preferred_element_type=jnp.float32).astype(jnp.bfloat16),
        "tp",
        scatter_dimension=0,
        tiled=True,
    ).astype(jnp.float32)
    power = jnp.mean(projected * projected, axis=-1, keepdims=True)
    middle = residual_rows + attn_gain * projected * lax.rsqrt(power + 1e-06)
    middle_power = jnp.mean(middle * middle, axis=-1, keepdims=True)
    normed = (mlp_gain * middle * lax.rsqrt(middle_power + 1e-06)).astype(jnp.bfloat16)
    normed_all = lax.all_gather(normed, "tp", axis=0, tiled=True)
    gate_full, up_full, down_full = collected
    gate_act = jnp.dot(normed_all, gate_full, preferred_element_type=jnp.float32)
    up_act = jnp.dot(normed_all, up_full, preferred_element_type=jnp.float32)
    hidden = (jax.nn.silu(gate_act) * up_act).astype(jnp.bfloat16)
    rows_slice = hidden
    lowered = lax.psum_scatter(
        jnp.dot(rows_slice, down_full, preferred_element_type=jnp.float32).astype(jnp.bfloat16),
        "tp",
        scatter_dimension=0,
        tiled=True,
    ).astype(jnp.float32)
    return (middle + 0.5 * lowered).astype(jnp.bfloat16)


GROUP = 4
PLANE = 4
MESH = pl.DeviceIdType.MESH
LOG2E = 1.4426950408889634
VMEM = pl.BlockSpec(memory_space=pltpu.VMEM)
ANY = pl.BlockSpec(memory_space=pl.ANY)
K, V, DOC, GATE, UP, DOWN, Q = range(7)


def remote(src, dst, send_sem, recv_sem, target):
    return pltpu.make_async_remote_copy(
        src_ref=src,
        dst_ref=dst,
        send_sem=send_sem,
        recv_sem=recv_sem,
        device_id=target,
        device_id_type=MESH,
    )


def span(index, width):
    return pl.ds(pl.multiple_of(index * width, width), width)


def layer_kernel(
    q_ref, k_ref, v_ref, d_ref, lg_ref, ow_hbm, resid_hbm, ag_ref, mg_ref, g_ref, u_ref, w_ref,
    out_ref,
    ow_ref, resid_ref,
    kall, vall, docs, qs, gkc, gw, uw, dw, att, arr, pbuf, pgot, mid, nall, hid, part, pair, red,
    got, comb,
    z_send, z_recv, p_send, p_recv, own_sem, load_sem, a_send, a_recv, t_send, t_recv,
    o_send, n_send, n_recv, f_send, f_recv, x_send, x_recv, r_send, r_recv, c_recv,
):
    me = lax.axis_index("sp")
    core = lax.axis_index("tp")
    z, p = me // PLANE, me % PLANE
    px, py = p % 2, p // 2
    other = 1 - core
    mate = (me, other)
    rows = k_ref.shape[0]
    qcols = q_ref.shape[1] // GROUP
    rank = qcols // HD
    fcols = g_ref.shape[1] // GROUP
    wrows, wcols = g_ref.shape[0], w_ref.shape[1]
    half, d_model = resid_hbm.shape
    coef = LOG2E / math.sqrt(HD)
    neighbours = (1, 2, 3)

    def peer(e):
        x = px if e == 2 else 1 - px
        y = py if e == 1 else 1 - py
        return y * 2 + x

    def near(e):
        return (z * PLANE + peer(e), core)

    def there(zb):
        return (zb * PLANE + p, core)

    def place(a, k):
        if a == K:
            return kall.at[span(k, rows)]
        if a == V:
            return vall.at[span(k, rows)]
        if a == DOC:
            return docs.at[k]
        if a == GATE:
            return gw.at[span(k, wrows)]
        if a == UP:
            return uw.at[span(k, wrows)]
        if a == DOWN:
            return dw.at[:, span(k, wcols)]
        return qs.at[k // PLANE]

    def piece(a, to):
        if a == K:
            return k_ref.at[:, span(to, HD)]
        if a == V:
            return v_ref.at[:, span(to, HD)]
        if a == DOC:
            return d_ref.at[...]
        if a == GATE:
            return g_ref.at[:, span(to, fcols)]
        if a == UP:
            return u_ref.at[:, span(to, fcols)]
        if a == DOWN:
            return w_ref.at[span(to, fcols)]
        return q_ref.at[:, span(to, qcols)]

    barrier = pltpu.get_barrier_semaphore()
    for d in range(1, GROUP):
        pl.semaphore_signal(barrier, inc=1, device_id=there((z + d) % GROUP), device_id_type=MESH)
    loads = (pltpu.make_async_copy(ow_hbm, ow_ref, load_sem.at[0]),
             pltpu.make_async_copy(resid_hbm, resid_ref, load_sem.at[1]))
    for e in neighbours:
        pl.semaphore_signal(barrier, inc=1, device_id=near(e), device_id_type=MESH)
    pl.semaphore_signal(barrier, inc=1, device_id=mate, device_id_type=MESH)
    pl.semaphore_wait(barrier, 7)

    def z_copy(a, to):
        return remote(piece(a, to), place(a, me), z_send.at[a, to], z_recv.at[a, z], there(to))

    def z_sends(a):
        for d in (1, 3, 2):
            z_copy(a, (z + d) % GROUP).start()

    def z_arrival(a, zs):
        at = place(a, zs * PLANE + p)
        remote(at, at, z_send.at[a, z], z_recv.at[a, zs], mate).wait_recv()

    def own_copy(a):
        return pltpu.make_async_copy(piece(a, z), place(a, me), own_sem.at[a])

    def p_copy(a, zs, e):
        at = place(a, zs * PLANE + p)
        return remote(at, at, p_send.at[a, zs, e - 1], p_recv.at[a, zs, e - 1], near(e))

    def p_own(a, e):
        return remote(piece(a, z), place(a, me), p_send.at[a, z, e - 1], p_recv.at[a, z, e - 1],
                      near(e))

    def p_arrival(a, zs, e):
        at = place(a, zs * PLANE + peer(e))
        remote(at, at, p_send.at[a, zs, e - 1], p_recv.at[a, zs, e - 1], mate).wait_recv()

    def spread_own(a):
        for e in neighbours:
            p_own(a, e).start()

    def forward(a, zs):
        z_arrival(a, zs)
        for e in neighbours:
            p_copy(a, zs, e).start()

    for a in (DOC, K, V, Q, GATE):
        z_sends(a)
    for a in (DOC, K, V):
        spread_own(a)
    for a in range(7):
        own_copy(a).start()
    for load in loads:
        load.start()

    lanes = 128

    def gate_row(r, at):
        block = lg_ref[:, at]
        chosen = lax.broadcasted_iota(jnp.int32, block.shape, 0) == z * rank + r
        return jnp.sum(jnp.where(chosen, block, 0.0), axis=0, keepdims=True) * LOG2E

    @pl.loop(0, kall.shape[0] // lanes)
    def _(j):
        at = span(j, lanes)
        for r in range(rank):
            row = gate_row(r, at)
            gkc[r, at, :] = jnp.transpose(jnp.broadcast_to(row, (lanes, lanes)))

    def ascending(i):
        return i + (i - z + GROUP) // GROUP

    def forwards(a):
        @pl.loop(0, GROUP - 1)
        def _(i):
            forward(a, ascending(i))

    forwards(DOC)

    @pl.loop(0, GROUP - 2)
    def _(i):
        forward(K, ascending(i))
        forward(V, ascending(i))

    for a in range(7):
        own_copy(a).wait()

    @pl.loop(0, GROUP)
    def _(zs):
        for e in neighbours:
            p_arrival(DOC, zs, e)

    every_doc = docs[...]

    def below(level):
        total = jnp.sum((every_doc < level).astype(jnp.float32), axis=0)
        return jnp.sum(total, axis=1, keepdims=True)

    first_of_1, first_of_2 = below(1), below(2)

    @pl.loop(0, GROUP)
    def _(zq):
        @pl.when(zq == 1)
        def _():
            forward(K, ascending(GROUP - 2))
            forward(V, ascending(GROUP - 2))
            spread_own(GATE)
            spread_own(UP)
            z_sends(UP)

        @pl.when(zq == GROUP - 1)
        def _():
            forwards(GATE)
            z_sends(DOWN)

        @pl.when(zq != z)
        def _():
            z_arrival(Q, zq)

        for e in neighbours:
            p_arrival(K, zq, e)
            p_arrival(V, zq, e)
        block = zq * PLANE + p
        q = jnp.concatenate([qs[zq, :, r * HD:(r + 1) * HD] for r in range(rank)], axis=0)
        own = span(block, rows)
        gq = jnp.concatenate([gate_row(r, own) for r in range(rank)], axis=1)
        dq = docs[block]
        start = jnp.where(dq == 0, 0.0, jnp.where(dq == 1, first_of_1, first_of_2))
        start = jnp.concatenate([start.astype(jnp.int32)] * rank, axis=1)
        qpos = block * rows + lax.broadcasted_iota(jnp.int32, (1, rows), 1)
        qpos = jnp.concatenate([qpos] * rank, axis=1)

        def attend(base, count, causal, state):
            m, l, acc = state
            at = pl.ds(pl.multiple_of(base, count), count)
            s = lax.dot_general(kall[at], q, (((1,), (1,)), ((), ())),
                                preferred_element_type=jnp.float32)
            gk = jnp.concatenate(
                [gkc[r, at, :] for r in range(rank) for _ in range(rows // lanes)], axis=1)
            s = (s * coef + gq) - gk
            kpos = base + lax.broadcasted_iota(jnp.int32, (count, 1), 0)
            seen = kpos >= start
            if causal:
                seen = seen & (kpos <= qpos)
            s = jnp.where(seen, s, jnp.float32(-1e30))
            m_new = jnp.maximum(m, jnp.max(s, axis=0, keepdims=True))
            prob = jnp.exp2(s - m_new)
            shrink = jnp.exp2(m - m_new)
            l = l * shrink + jnp.sum(prob, axis=0, keepdims=True)
            acc = acc * shrink + lax.dot_general(
                vall[at], prob.astype(jnp.bfloat16), (((0,), (0,)), ((), ())),
                preferred_element_type=jnp.float32)
            return m_new, l, acc

        wide = 2 * rows
        state = (jnp.full((1, rank * rows), -1e20, jnp.float32),
                 jnp.zeros((1, rank * rows), jnp.float32),
                 jnp.zeros((HD, rank * rows), jnp.float32))
        state = lax.fori_loop(0, 2 * zq, lambda i, s: attend(i * wide, wide, False, s), state)
        m, l, acc = lax.fori_loop(
            0, p + 1, lambda i, s: attend((zq * PLANE + i) * rows, rows, True, s), state)
        res = acc / l
        for r in range(rank):
            att[zq, :, r * HD:(r + 1) * HD] = jnp.transpose(
                res[:, r * rows:(r + 1) * rows]).astype(jnp.bfloat16)

        @pl.when(zq != z)
        def _():
            remote(att.at[zq], arr.at[z], a_send.at[zq], a_recv.at[z], there(zq)).start()

    forwards(UP)
    spread_own(DOWN)
    for load in loads:
        load.wait()
    own = pltpu.make_async_copy(att.at[z], arr.at[z], own_sem.at[0])
    own.start()
    own.wait()
    for d in range(1, GROUP):
        zs = (z + d) % GROUP
        at = arr.at[zs]
        remote(at, at, a_send.at[zs], a_recv.at[zs], mate).wait_recv()
    tile = 512

    @pl.loop(0, d_model // tile)
    def _(j):
        at = span(j, tile)
        total = jnp.dot(arr[0], ow_ref[0:qcols, at], preferred_element_type=jnp.float32)
        for g in range(1, GROUP):
            total += jnp.dot(arr[g], ow_ref[g * qcols:(g + 1) * qcols, at],
                             preferred_element_type=jnp.float32)
        pbuf[0, :, at] = total[:half].astype(jnp.bfloat16)
        pbuf[1, :, at] = total[half:].astype(jnp.bfloat16)

    swap = remote(pbuf.at[other], pgot, t_send, t_recv, mate)
    swap.start()
    swap.wait()
    projected = pbuf[core].astype(jnp.float32) + pgot[...].astype(jnp.float32)
    power = jnp.mean(projected * projected, axis=-1, keepdims=True)
    middle = resid_ref[...].astype(jnp.float32) + ag_ref[...] * projected * lax.rsqrt(power + 1e-06)
    mid[...] = middle
    mpower = jnp.mean(middle * middle, axis=-1, keepdims=True)
    nall[z, core] = (mg_ref[...] * middle * lax.rsqrt(mpower + 1e-06)).astype(jnp.bfloat16)

    piece_rows = half // 2

    def relay(zb, side, c, send_sem):
        block = nall.at[zb, core, span(c, piece_rows)]
        return remote(block, block, send_sem, n_recv.at[zb, c],
                      ((z + 1 - 2 * side) * PLANE + p, core))

    def share(zb, c):
        block = nall.at[zb, core, span(c, piece_rows)]
        return remote(block, block, f_send.at[zb, c], f_recv.at[zb, c], mate)

    def shared(zb, c):
        over = nall.at[zb, other, span(c, piece_rows)]
        remote(over, over, f_send.at[zb, c], f_recv.at[zb, c], mate).wait_recv()

    def onward(side):
        return (side == 0) & (z < GROUP - 1) | (side == 1) & (z > 0)

    for c in (0, 1):
        for side in (0, 1):
            @pl.when(onward(side))
            def _():
                relay(z, side, c, o_send.at[side, c]).start()
    for c in (0, 1):
        share(z, c).start()

    def arrive(d, c):
        for side in (0, 1):
            zb = z - d if side == 0 else z + d

            @pl.when((zb >= 0) & (zb < GROUP))
            def _():
                block = nall.at[zb, core, span(c, piece_rows)]
                remote(block, block, n_send.at[zb, c], n_recv.at[zb, c], mate).wait_recv()
                @pl.when(onward(side))
                def _():
                    relay(zb, side, c, n_send.at[zb, c]).start()
                share(zb, c).start()

    mate_z = z + 1 - 2 * (z % 2)
    far = GROUP // 2 - (z // 2) * 2
    at_end = (z == 0) | (z == GROUP - 1)

    def expand(zb, c):
        shared(zb, c)
        rows_in = jnp.concatenate(
            [nall[zb, i, span(c, piece_rows), :] for i in (0, 1)], axis=0)
        ftile = 256
        for j in range(fcols // ftile):
            at = slice(j * ftile, (j + 1) * ftile)
            gate = jnp.dot(rows_in, gw[:, at], preferred_element_type=jnp.float32)
            up = jnp.dot(rows_in, uw[:, at], preferred_element_type=jnp.float32)
            hid[zb, c, :, at] = (gate / (1.0 + jnp.exp(-gate)) * up).astype(jnp.bfloat16)

    gcols = PLANE * wcols
    hcols = d_model // 2

    def trade(zb, g):
        at = span(g, gcols)
        return remote(part.at[zb, other, :, at], pair.at[zb, :, at], x_send.at[zb, g],
                      x_recv.at[zb, g], mate)

    def lower(zb, g):
        at = span(g, gcols)
        rows_in = jnp.concatenate([hid[zb, 0], hid[zb, 1]], axis=0)
        total = jnp.dot(rows_in, dw[:, at], preferred_element_type=jnp.float32)
        for c in (0, 1):
            for i in (0, 1):
                first = (2 * c + i) * piece_rows
                part[zb, i, c * piece_rows:(c + 1) * piece_rows, at] = (
                    total[first:first + piece_rows].astype(jnp.bfloat16))
        trade(zb, g).start()

    def both(zb, at):
        return part[zb, core, :, at].astype(jnp.float32) + pair[zb, :, at].astype(jnp.float32)

    def give(zb, g):
        at = span(g, gcols)
        return remote(red.at[zb, :, at], got.at[0, :, at], r_send.at[zb, g], r_recv.at[0, g],
                      there(zb))

    def corner(c, h):
        return span(c, piece_rows), slice(h * hcols, (h + 1) * hcols)

    def trade_far(zb, c, h):
        rs, cs = corner(c, h)
        return remote(part.at[zb, other, rs, cs], pair.at[zb, rs, cs], x_send.at[zb, 2 * c + h],
                      x_recv.at[zb, 2 * c + h], mate)

    def give_far(zb, c, h):
        rs, cs = corner(c, h)
        return remote(red.at[zb, rs, cs], got.at[1, rs, cs], r_send.at[zb, 2 * c + h],
                      r_recv.at[1, 2 * c + h], there(zb))

    def give_comb(t, zb, c, h):
        rs, cs = corner(c, h)
        return remote(red.at[zb, rs, cs], comb.at[t, rs, cs], r_send.at[zb, 2 * c + h],
                      c_recv.at[t, 2 * c + h], there(mate_z))

    def both_far(zb, rs, cs):
        return part[zb, core, rs, cs].astype(jnp.float32) + pair[zb, rs, cs].astype(jnp.float32)

    forwards(DOWN)
    arrive(1, 0)
    arrive(1, 1)

    @pl.loop(0, GROUP)
    def _(zs):
        for a in (GATE, UP):
            for e in neighbours:
                p_arrival(a, zs, e)

    @pl.loop(0, 2)
    def _(c):
        expand(mate_z, c)
        arrive(2, c)

    @pl.loop(0, GROUP + 1)
    def _(s):
        @pl.when(s < GROUP)
        def _():
            for e in neighbours:
                p_arrival(DOWN, s, e)
            lower(mate_z, s)

        @pl.when(s > 0)
        def _():
            at = span(s - 1, gcols)
            trade(mate_z, s - 1).wait()
            red[mate_z, :, at] = both(mate_z, at).astype(jnp.bfloat16)
            give(mate_z, s - 1).start()

    def far_block(t):
        return far + t + (1 - 2 * t) * (z // 2)

    def send_far(t):
        zb = far_block(t)

        @pl.loop(0, 2)
        def _(c):
            if t == 1:
                arrive(3, c)
            expand(zb, c)
            for h in (0, 1):
                rs, cs = corner(c, h)
                total = jnp.dot(hid[zb, c], dw[:, cs], preferred_element_type=jnp.float32)
                for i in (0, 1):
                    part[zb, i, rs, cs] = total[i * piece_rows:(i + 1) * piece_rows].astype(
                        jnp.bfloat16)
                trade_far(zb, c, h).start()
            for h in (0, 1):
                rs, cs = corner(c, h)
                trade_far(zb, c, h).wait()

                @pl.when(at_end)
                def _():
                    red[zb, rs, cs] = both_far(zb, rs, cs).astype(jnp.bfloat16)
                    give_comb(t, zb, c, h).start()

    def combine(t):
        zb = far_block(t)

        @pl.when((z > 0) & (z < GROUP - 1))
        def _():
            @pl.loop(0, 2)
            def _(c):
                for h in (0, 1):
                    rs, cs = corner(c, h)
                    give_comb(t, zb, c, h).wait_recv()
                    red[zb, rs, cs] = (both_far(zb, rs, cs)
                                       + comb[t, rs, cs].astype(jnp.float32)).astype(jnp.bfloat16)
                    give_far(zb, c, h).start()

    send_far(0)
    send_far(1)
    combine(0)

    @pl.loop(0, 2)
    def _(c):
        expand(z, c)

    @pl.loop(0, GROUP)
    def _(g):
        lower(z, g)

    combine(1)

    @pl.loop(0, GROUP)
    def _(g):
        trade(z, g).wait()

    for c in (0, 1):
        for h in (0, 1):
            give_far(far, c, h).wait_recv()

    @pl.loop(0, GROUP)
    def _(g):
        at = span(g, gcols)
        give(mate_z, g).wait_recv()
        total = both(z, at) + got[0, :, at].astype(jnp.float32) + got[1, :, at].astype(jnp.float32)
        out_ref[:, at] = (mid[:, at] + 0.5 * total).astype(jnp.bfloat16)

    for d in range(1, GROUP):
        zb = (z + d) % GROUP
        for a in range(7):
            z_copy(a, zb).wait_send()
        remote(att.at[zb], arr.at[z], a_send.at[zb], a_recv.at[z], there(zb)).wait_send()

        @pl.loop(0, GROUP)
        def _(g):
            give(zb, g).wait_send()

    for a in range(6):
        for e in neighbours:
            p_own(a, e).wait_send()
            for d in range(1, GROUP):
                p_copy(a, (z + d) % GROUP, e).wait_send()
    for c in (0, 1):
        share(z, c).wait_send()
        for side in (0, 1):
            @pl.when(onward(side))
            def _():
                relay(z, side, c, o_send.at[side, c]).wait_send()
        for d in range(1, GROUP):
            share((z + d) % GROUP, c).wait_send()
            for side in (0, 1):
                zb = z - d if side == 0 else z + d

                @pl.when((zb >= 0) & (zb < GROUP) & onward(side))
                def _():
                    relay(zb, side, c, n_send.at[zb, c]).wait_send()


def grouped(
    sp, resid, queries, keys, values, log_gates, documents, out_weight, attn_gain, mlp_gain,
    gate_weight, up_weight, down_weight,
):
    rows, ff = keys.shape[0], gate_weight.shape[1] // GROUP
    half, d_model = resid.shape
    tokens = rows * sp
    qcols = queries.shape[1] // GROUP
    rank = qcols // HD
    bf, f32 = jnp.bfloat16, jnp.float32
    dma = pltpu.SemaphoreType.DMA
    return pl.pallas_call(
        layer_kernel,
        out_shape=jax.ShapeDtypeStruct(resid.shape, bf),
        in_specs=[VMEM] * 5 + [ANY] * 2 + [VMEM] * 2 + [ANY] * 3,
        out_specs=VMEM,
        scratch_shapes=[
            pltpu.VMEM(out_weight.shape, bf),
            pltpu.VMEM(resid.shape, bf),
            pltpu.VMEM((tokens, HD), bf),
            pltpu.VMEM((tokens, HD), bf),
            pltpu.VMEM((sp, 1, rows), jnp.int32),
            pltpu.VMEM((GROUP, rows, qcols), bf),
            pltpu.VMEM((rank, tokens, 128), f32),
            pltpu.VMEM((d_model, ff), bf),
            pltpu.VMEM((d_model, ff), bf),
            pltpu.VMEM((ff, d_model), bf),
            pltpu.VMEM((GROUP, rows, qcols), bf),
            pltpu.VMEM((GROUP, rows, qcols), bf),
            pltpu.VMEM((2, half, d_model), bf),
            pltpu.VMEM((half, d_model), bf),
            pltpu.VMEM((half, d_model), f32),
            pltpu.VMEM((GROUP, 2, half, d_model), bf),
            pltpu.VMEM((GROUP, 2, half, ff), bf),
            pltpu.VMEM((GROUP, 2, half, d_model), bf),
            pltpu.VMEM((GROUP, half, d_model), bf),
            pltpu.VMEM((GROUP, half, d_model), bf),
            pltpu.VMEM((2, half, d_model), bf),
            pltpu.VMEM((2, half, d_model), bf),
            dma((7, GROUP)), dma((7, GROUP)), dma((6, GROUP, 3)), dma((6, GROUP, 3)), dma((7,)),
            dma((2,)),
            dma((GROUP,)), dma((GROUP,)), dma, dma,
            dma((2, 2)), dma((GROUP, 2)), dma((GROUP, 2)), dma((GROUP, 2)), dma((GROUP, 2)),
            dma((GROUP, GROUP)), dma((GROUP, GROUP)), dma((GROUP, GROUP)), dma((2, GROUP)),
            dma((2, GROUP)),
        ],
        compiler_params=pltpu.CompilerParams(
            collective_id=0, has_side_effects=True, vmem_limit_bytes=62 * 1024 * 1024),
    )(queries, keys, values, documents[None, :], log_gates,
      out_weight, resid, attn_gain[None, :], mlp_gain[None, :], gate_weight, up_weight,
      down_weight)


def solution(mesh):
    placed = (
        P(("sp", "tp"), None),
        P("sp", "tp"),
        P("sp", "tp"),
        P("sp", "tp"),
        P("tp", None),
        P("sp"),
        P("tp", None),
        P(),
        P(),
        P("sp", "tp"),
        P("sp", "tp"),
        P("tp", "sp"),
    )
    sp, tp = mesh.shape["sp"], mesh.shape["tp"]

    def layer(*args):
        kv_dev = args[2].shape[1] // HD
        fits = tp == 2 and sp == GROUP * PLANE and kv_dev == GROUP
        return grouped(sp, *args) if fits else local(*args)

    return jax.shard_map(
        layer, mesh=mesh, in_specs=placed, out_specs=P(("sp", "tp"), None), check_vma=False
    )
```

```python
import math

import jax
import jax.numpy as jnp
from jax import lax
from jax.experimental import pallas as pl
from jax.experimental.pallas import tpu as pltpu
from jax.sharding import PartitionSpec as P

HD = 128


def local(
    resid,
    queries,
    keys,
    values,
    log_gates,
    documents,
    out_weight,
    attn_gain,
    mlp_gain,
    gate_weight,
    up_weight,
    down_weight,
):
    tok_rows = queries.shape[0]
    kv_dev = keys.shape[1] // HD
    heads_dev = log_gates.shape[0]
    group_size = heads_dev // kv_dev
    score_scale = 1.0 / math.sqrt(HD)
    own_start = lax.axis_index("sp") * tok_rows
    own_last = own_start + tok_rows - 1
    first_doc = documents[0]
    query_pos = own_start + lax.iota(jnp.int32, tok_rows)
    query_heads = queries.reshape(tok_rows, kv_dev, group_size, HD)
    key_gates_all = log_gates.reshape(kv_dev, group_size, log_gates.shape[1])
    query_gates = lax.dynamic_slice_in_dim(key_gates_all, own_start, tok_rows, 2)
    collected = (
        lax.all_gather(gate_weight, "sp", axis=0, tiled=True),
        lax.all_gather(up_weight, "sp", axis=0, tiled=True),
        lax.all_gather(down_weight, "sp", axis=1, tiled=True),
    )
    residual_rows = resid.astype(jnp.float32)

    def attend_block(running, key_rows, value_rows, doc_rows, first_row):
        run_max, run_sum, accumulated = running
        key_count = key_rows.shape[0]
        scores = (
            jnp.einsum(
                "tkgd,skd->kgts",
                query_heads,
                key_rows.reshape(key_count, kv_dev, HD),
                preferred_element_type=jnp.float32,
            )
            * score_scale
        )
        key_gates = lax.dynamic_slice_in_dim(key_gates_all, first_row, key_count, 2)
        scores = scores + query_gates[..., None] - key_gates[:, :, None, :]
        key_pos = first_row + lax.iota(jnp.int32, key_count)
        visible = (key_pos[None, :] <= query_pos[:, None]) & (
            doc_rows[None, :] == documents[:, None]
        )
        scores = jnp.where(visible, scores, jnp.float32(-1e30))
        new_max = jnp.maximum(run_max, jnp.max(scores, axis=-1))
        probs = jnp.where(visible, jnp.exp(scores - new_max[..., None]), jnp.float32(0.0))
        shrink = jnp.exp(run_max - new_max)
        run_sum = run_sum * shrink + jnp.sum(probs, axis=-1)
        weighted = jnp.einsum(
            "kgts,skd->kgtd",
            probs.astype(jnp.bfloat16),
            value_rows.reshape(key_count, kv_dev, HD),
            preferred_element_type=jnp.float32,
        )
        accumulated = accumulated * shrink[..., None] + weighted
        return (new_max, run_sum, accumulated)

    def maybe_attend(running, key_rows, value_rows, doc_rows, first_row):
        needed = (first_row <= own_last) & (doc_rows[-1] >= first_doc)

        def compute(state):
            return attend_block(state, key_rows, value_rows, doc_rows, first_row)

        def keep(state):
            return state

        return lax.cond(needed, compute, keep, running)

    start_state = (
        jnp.full((kv_dev, group_size, tok_rows), -1e30, jnp.float32),
        jnp.zeros((kv_dev, group_size, tok_rows), jnp.float32),
        jnp.zeros((kv_dev, group_size, tok_rows, HD), jnp.float32),
    )
    key_rows = lax.all_gather(keys, "sp", axis=0, tiled=True)
    value_rows = lax.all_gather(values, "sp", axis=0, tiled=True)
    doc_rows = lax.all_gather(documents, "sp", axis=0, tiled=True)
    key_count = key_rows.shape[0]
    block_len = math.gcd(key_count, 1024)

    def advance(block_index, inner):
        offset = block_index * block_len
        return maybe_attend(
            inner,
            lax.dynamic_slice_in_dim(key_rows, offset, block_len, 0),
            lax.dynamic_slice_in_dim(value_rows, offset, block_len, 0),
            lax.dynamic_slice_in_dim(doc_rows, offset, block_len, 0),
            offset,
        )

    run_max, run_sum, accumulated = lax.fori_loop(0, key_count // block_len, advance, start_state)
    attended = accumulated / run_sum[..., None]
    attended = (
        jnp.transpose(attended, (2, 0, 1, 3)).reshape(tok_rows, heads_dev * HD).astype(jnp.bfloat16)
    )
    rows_slice = attended
    projected = lax.psum_scatter(
        jnp.dot(rows_slice, out_weight, preferred_element_type=jnp.float32).astype(jnp.bfloat16),
        "tp",
        scatter_dimension=0,
        tiled=True,
    ).astype(jnp.float32)
    power = jnp.mean(projected * projected, axis=-1, keepdims=True)
    middle = residual_rows + attn_gain * projected * lax.rsqrt(power + 1e-06)
    middle_power = jnp.mean(middle * middle, axis=-1, keepdims=True)
    normed = (mlp_gain * middle * lax.rsqrt(middle_power + 1e-06)).astype(jnp.bfloat16)
    normed_all = lax.all_gather(normed, "tp", axis=0, tiled=True)
    gate_full, up_full, down_full = collected
    gate_act = jnp.dot(normed_all, gate_full, preferred_element_type=jnp.float32)
    up_act = jnp.dot(normed_all, up_full, preferred_element_type=jnp.float32)
    hidden = (jax.nn.silu(gate_act) * up_act).astype(jnp.bfloat16)
    rows_slice = hidden
    lowered = lax.psum_scatter(
        jnp.dot(rows_slice, down_full, preferred_element_type=jnp.float32).astype(jnp.bfloat16),
        "tp",
        scatter_dimension=0,
        tiled=True,
    ).astype(jnp.float32)
    return (middle + 0.5 * lowered).astype(jnp.bfloat16)


GROUP = 4
PLANE = 4
MESH = pl.DeviceIdType.MESH
LOG2E = 1.4426950408889634
VMEM = pl.BlockSpec(memory_space=pltpu.VMEM)
ANY = pl.BlockSpec(memory_space=pl.ANY)
K, V, DOC, GATE, UP, DOWN, Q = range(7)


def remote(src, dst, send_sem, recv_sem, target):
    return pltpu.make_async_remote_copy(
        src_ref=src,
        dst_ref=dst,
        send_sem=send_sem,
        recv_sem=recv_sem,
        device_id=target,
        device_id_type=MESH,
    )


def span(index, width):
    return pl.ds(pl.multiple_of(index * width, width), width)


def layer_kernel(
    q_ref, k_ref, v_ref, d_ref, lg_ref, ow_hbm, resid_hbm, ag_ref, mg_ref, g_ref, u_ref, w_ref,
    out_ref,
    ow_ref, resid_ref,
    kall, vall, docs, qs, gkc, gw, uw, dw, att, arr, pbuf, pgot, mid, nall, hid, part, pair, red,
    got, comb,
    z_send, z_recv, p_send, p_recv, own_sem, load_sem, a_send, a_recv, t_send, t_recv,
    o_send, n_send, n_recv, f_send, f_recv, x_send, x_recv, r_send, r_recv, c_recv,
):
    me = lax.axis_index("sp")
    core = lax.axis_index("tp")
    z, p = me // PLANE, me % PLANE
    px, py = p % 2, p // 2
    other = 1 - core
    mate = (me, other)
    rows = k_ref.shape[0]
    qcols = q_ref.shape[1] // GROUP
    rank = qcols // HD
    fcols = g_ref.shape[1] // GROUP
    wrows, wcols = g_ref.shape[0], w_ref.shape[1]
    half, d_model = resid_hbm.shape
    coef = LOG2E / math.sqrt(HD)
    neighbours = (1, 2, 3)

    def peer(e):
        x = px if e == 2 else 1 - px
        y = py if e == 1 else 1 - py
        return y * 2 + x

    def near(e):
        return (z * PLANE + peer(e), core)

    def there(zb):
        return (zb * PLANE + p, core)

    def place(a, k):
        if a == K:
            return kall.at[span(k, rows)]
        if a == V:
            return vall.at[span(k, rows)]
        if a == DOC:
            return docs.at[k]
        if a == GATE:
            return gw.at[span(k, wrows)]
        if a == UP:
            return uw.at[span(k, wrows)]
        if a == DOWN:
            return dw.at[:, span(k, wcols)]
        return qs.at[k // PLANE]

    def piece(a, to):
        if a == K:
            return k_ref.at[:, span(to, HD)]
        if a == V:
            return v_ref.at[:, span(to, HD)]
        if a == DOC:
            return d_ref.at[...]
        if a == GATE:
            return g_ref.at[:, span(to, fcols)]
        if a == UP:
            return u_ref.at[:, span(to, fcols)]
        if a == DOWN:
            return w_ref.at[span(to, fcols)]
        return q_ref.at[:, span(to, qcols)]

    barrier = pltpu.get_barrier_semaphore()
    for d in range(1, GROUP):
        pl.semaphore_signal(barrier, inc=1, device_id=there((z + d) % GROUP), device_id_type=MESH)
    loads = (pltpu.make_async_copy(ow_hbm, ow_ref, load_sem.at[0]),
             pltpu.make_async_copy(resid_hbm, resid_ref, load_sem.at[1]))
    for e in neighbours:
        pl.semaphore_signal(barrier, inc=1, device_id=near(e), device_id_type=MESH)
    pl.semaphore_signal(barrier, inc=1, device_id=mate, device_id_type=MESH)
    lanes = 128

    def gate_row(r, at):
        block = lg_ref[:, at]
        chosen = lax.broadcasted_iota(jnp.int32, block.shape, 0) == z * rank + r
        return jnp.sum(jnp.where(chosen, block, 0.0), axis=0, keepdims=True) * LOG2E

    @pl.loop(0, kall.shape[0] // lanes)
    def _(j):
        at = span(j, lanes)
        for r in range(rank):
            row = gate_row(r, at)
            gkc[r, at, :] = jnp.transpose(jnp.broadcast_to(row, (lanes, lanes)))

    pl.semaphore_wait(barrier, 7)

    def z_copy(a, to):
        return remote(piece(a, to), place(a, me), z_send.at[a, to], z_recv.at[a, z], there(to))

    def z_sends(a):
        for d in (1, 3, 2):
            z_copy(a, (z + d) % GROUP).start()

    def z_arrival(a, zs):
        at = place(a, zs * PLANE + p)
        remote(at, at, z_send.at[a, z], z_recv.at[a, zs], mate).wait_recv()

    def own_copy(a):
        return pltpu.make_async_copy(piece(a, z), place(a, me), own_sem.at[a])

    def p_copy(a, zs, e):
        at = place(a, zs * PLANE + p)
        return remote(at, at, p_send.at[a, zs, e - 1], p_recv.at[a, zs, e - 1], near(e))

    def p_own(a, e):
        return remote(piece(a, z), place(a, me), p_send.at[a, z, e - 1], p_recv.at[a, z, e - 1],
                      near(e))

    def p_arrival(a, zs, e):
        at = place(a, zs * PLANE + peer(e))
        remote(at, at, p_send.at[a, zs, e - 1], p_recv.at[a, zs, e - 1], mate).wait_recv()

    def spread_own(a):
        for e in neighbours:
            p_own(a, e).start()

    def forward(a, zs):
        z_arrival(a, zs)
        for e in neighbours:
            p_copy(a, zs, e).start()

    for a in (DOC, K, V, Q, GATE):
        z_sends(a)
    for a in (DOC, K, V):
        spread_own(a)
    for a in range(7):
        own_copy(a).start()
    for load in loads:
        load.start()

    def ascending(i):
        return i + (i - z + GROUP) // GROUP

    def forwards(a):
        @pl.loop(0, GROUP - 1)
        def _(i):
            forward(a, ascending(i))

    forwards(DOC)

    @pl.loop(0, GROUP - 2)
    def _(i):
        forward(K, ascending(i))
        forward(V, ascending(i))

    for a in range(7):
        own_copy(a).wait()

    @pl.loop(0, GROUP)
    def _(zs):
        for e in neighbours:
            p_arrival(DOC, zs, e)

    every_doc = docs[...]

    def below(level):
        total = jnp.sum((every_doc < level).astype(jnp.float32), axis=0)
        return jnp.sum(total, axis=1, keepdims=True)

    first_of_1, first_of_2 = below(1), below(2)

    @pl.loop(0, GROUP)
    def _(zq):
        @pl.when(zq == 1)
        def _():
            forward(K, ascending(GROUP - 2))
            forward(V, ascending(GROUP - 2))
            spread_own(GATE)
            spread_own(UP)
            z_sends(UP)

        @pl.when(zq == GROUP - 1)
        def _():
            forwards(GATE)
            z_sends(DOWN)

        @pl.when(zq != z)
        def _():
            z_arrival(Q, zq)

        for e in neighbours:
            p_arrival(K, zq, e)
            p_arrival(V, zq, e)
        block = zq * PLANE + p
        q = jnp.concatenate([qs[zq, :, r * HD:(r + 1) * HD] for r in range(rank)], axis=0)
        own = span(block, rows)
        gq = jnp.concatenate([gate_row(r, own) for r in range(rank)], axis=1)
        dq = docs[block]
        start = jnp.where(dq == 0, 0.0, jnp.where(dq == 1, first_of_1, first_of_2))
        start = jnp.concatenate([start.astype(jnp.int32)] * rank, axis=1)
        qpos = block * rows + lax.broadcasted_iota(jnp.int32, (1, rows), 1)
        qpos = jnp.concatenate([qpos] * rank, axis=1)

        def attend(base, count, causal, state):
            m, l, acc = state
            at = pl.ds(pl.multiple_of(base, count), count)
            s = lax.dot_general(kall[at], q, (((1,), (1,)), ((), ())),
                                preferred_element_type=jnp.float32)
            gk = jnp.concatenate(
                [gkc[r, at, :] for r in range(rank) for _ in range(rows // lanes)], axis=1)
            s = (s * coef + gq) - gk
            kpos = base + lax.broadcasted_iota(jnp.int32, (count, 1), 0)
            seen = kpos >= start
            if causal:
                seen = seen & (kpos <= qpos)
            s = jnp.where(seen, s, jnp.float32(-1e30))
            m_new = jnp.maximum(m, jnp.max(s, axis=0, keepdims=True))
            prob = jnp.exp2(s - m_new)
            shrink = jnp.exp2(m - m_new)
            l = l * shrink + jnp.sum(prob, axis=0, keepdims=True)
            acc = acc * shrink + lax.dot_general(
                vall[at], prob.astype(jnp.bfloat16), (((0,), (0,)), ((), ())),
                preferred_element_type=jnp.float32)
            return m_new, l, acc

        wide = 2 * rows
        state = (jnp.full((1, rank * rows), -1e20, jnp.float32),
                 jnp.zeros((1, rank * rows), jnp.float32),
                 jnp.zeros((HD, rank * rows), jnp.float32))
        state = lax.fori_loop(0, 2 * zq, lambda i, s: attend(i * wide, wide, False, s), state)
        m, l, acc = lax.fori_loop(
            0, p + 1, lambda i, s: attend((zq * PLANE + i) * rows, rows, True, s), state)
        res = acc / l
        for r in range(rank):
            att[zq, :, r * HD:(r + 1) * HD] = jnp.transpose(
                res[:, r * rows:(r + 1) * rows]).astype(jnp.bfloat16)

        @pl.when(zq != z)
        def _():
            remote(att.at[zq], arr.at[z], a_send.at[zq], a_recv.at[z], there(zq)).start()

    forwards(UP)
    spread_own(DOWN)
    for load in loads:
        load.wait()
    own = pltpu.make_async_copy(att.at[z], arr.at[z], own_sem.at[0])
    own.start()
    own.wait()
    for d in range(1, GROUP):
        zs = (z + d) % GROUP
        at = arr.at[zs]
        remote(at, at, a_send.at[zs], a_recv.at[zs], mate).wait_recv()
    tile = 512

    @pl.loop(0, d_model // tile)
    def _(j):
        at = span(j, tile)
        total = jnp.dot(arr[0], ow_ref[0:qcols, at], preferred_element_type=jnp.float32)
        for g in range(1, GROUP):
            total += jnp.dot(arr[g], ow_ref[g * qcols:(g + 1) * qcols, at],
                             preferred_element_type=jnp.float32)
        pbuf[0, :, at] = total[:half].astype(jnp.bfloat16)
        pbuf[1, :, at] = total[half:].astype(jnp.bfloat16)

    swap = remote(pbuf.at[other], pgot, t_send, t_recv, mate)
    swap.start()
    swap.wait()
    projected = pbuf[core].astype(jnp.float32) + pgot[...].astype(jnp.float32)
    power = jnp.mean(projected * projected, axis=-1, keepdims=True)
    middle = resid_ref[...].astype(jnp.float32) + ag_ref[...] * projected * lax.rsqrt(power + 1e-06)
    mid[...] = middle
    mpower = jnp.mean(middle * middle, axis=-1, keepdims=True)
    nall[z, core] = (mg_ref[...] * middle * lax.rsqrt(mpower + 1e-06)).astype(jnp.bfloat16)

    piece_rows = half // 2

    def relay(zb, side, c, send_sem):
        block = nall.at[zb, core, span(c, piece_rows)]
        return remote(block, block, send_sem, n_recv.at[zb, c],
                      ((z + 1 - 2 * side) * PLANE + p, core))

    def share(zb, c):
        block = nall.at[zb, core, span(c, piece_rows)]
        return remote(block, block, f_send.at[zb, c], f_recv.at[zb, c], mate)

    def shared(zb, c):
        over = nall.at[zb, other, span(c, piece_rows)]
        remote(over, over, f_send.at[zb, c], f_recv.at[zb, c], mate).wait_recv()

    def onward(side):
        return (side == 0) & (z < GROUP - 1) | (side == 1) & (z > 0)

    for c in (0, 1):
        for side in (0, 1):
            @pl.when(onward(side))
            def _():
                relay(z, side, c, o_send.at[side, c]).start()
    for c in (0, 1):
        share(z, c).start()

    def arrive(d, c):
        for side in (0, 1):
            zb = z - d if side == 0 else z + d

            @pl.when((zb >= 0) & (zb < GROUP))
            def _():
                block = nall.at[zb, core, span(c, piece_rows)]
                remote(block, block, n_send.at[zb, c], n_recv.at[zb, c], mate).wait_recv()
                @pl.when(onward(side))
                def _():
                    relay(zb, side, c, n_send.at[zb, c]).start()
                share(zb, c).start()

    mate_z = z + 1 - 2 * (z % 2)
    far = GROUP // 2 - (z // 2) * 2
    at_end = (z == 0) | (z == GROUP - 1)

    def expand(zb, c):
        shared(zb, c)
        rows_in = jnp.concatenate(
            [nall[zb, i, span(c, piece_rows), :] for i in (0, 1)], axis=0)
        ftile = 256
        for j in range(fcols // ftile):
            at = slice(j * ftile, (j + 1) * ftile)
            gate = jnp.dot(rows_in, gw[:, at], preferred_element_type=jnp.float32)
            up = jnp.dot(rows_in, uw[:, at], preferred_element_type=jnp.float32)
            hid[zb, c, :, at] = (gate / (1.0 + jnp.exp(-gate)) * up).astype(jnp.bfloat16)

    gcols = PLANE * wcols
    hcols = d_model // 2

    def trade(zb, g):
        at = span(g, gcols)
        return remote(part.at[zb, other, :, at], pair.at[zb, :, at], x_send.at[zb, g],
                      x_recv.at[zb, g], mate)

    def lower(zb, g):
        at = span(g, gcols)
        rows_in = jnp.concatenate([hid[zb, 0], hid[zb, 1]], axis=0)
        total = jnp.dot(rows_in, dw[:, at], preferred_element_type=jnp.float32)
        for c in (0, 1):
            for i in (0, 1):
                first = (2 * c + i) * piece_rows
                part[zb, i, c * piece_rows:(c + 1) * piece_rows, at] = (
                    total[first:first + piece_rows].astype(jnp.bfloat16))
        trade(zb, g).start()

    def both(zb, at):
        return part[zb, core, :, at].astype(jnp.float32) + pair[zb, :, at].astype(jnp.float32)

    def give(zb, g):
        at = span(g, gcols)
        return remote(red.at[zb, :, at], got.at[0, :, at], r_send.at[zb, g], r_recv.at[0, g],
                      there(zb))

    def corner(c, h):
        return span(c, piece_rows), slice(h * hcols, (h + 1) * hcols)

    def trade_far(zb, c, h):
        rs, cs = corner(c, h)
        return remote(part.at[zb, other, rs, cs], pair.at[zb, rs, cs], x_send.at[zb, 2 * c + h],
                      x_recv.at[zb, 2 * c + h], mate)

    def give_far(zb, c, h):
        rs, cs = corner(c, h)
        return remote(red.at[zb, rs, cs], got.at[1, rs, cs], r_send.at[zb, 2 * c + h],
                      r_recv.at[1, 2 * c + h], there(zb))

    def give_comb(t, zb, c, h):
        rs, cs = corner(c, h)
        return remote(red.at[zb, rs, cs], comb.at[t, rs, cs], r_send.at[zb, 2 * c + h],
                      c_recv.at[t, 2 * c + h], there(mate_z))

    def both_far(zb, rs, cs):
        return part[zb, core, rs, cs].astype(jnp.float32) + pair[zb, rs, cs].astype(jnp.float32)

    forwards(DOWN)
    arrive(1, 0)
    arrive(1, 1)

    @pl.loop(0, GROUP)
    def _(zs):
        for a in (GATE, UP):
            for e in neighbours:
                p_arrival(a, zs, e)

    @pl.loop(0, 2)
    def _(c):
        expand(mate_z, c)
        arrive(2, c)

    @pl.loop(0, GROUP + 1)
    def _(s):
        @pl.when(s < GROUP)
        def _():
            for e in neighbours:
                p_arrival(DOWN, s, e)
            lower(mate_z, s)

        @pl.when(s > 0)
        def _():
            at = span(s - 1, gcols)
            trade(mate_z, s - 1).wait()
            red[mate_z, :, at] = both(mate_z, at).astype(jnp.bfloat16)
            give(mate_z, s - 1).start()

    def far_block(t):
        return far + t + (1 - 2 * t) * (z // 2)

    def send_far(t):
        zb = far_block(t)

        @pl.loop(0, 2)
        def _(c):
            if t == 1:
                arrive(3, c)
            expand(zb, c)
            for h in (0, 1):
                rs, cs = corner(c, h)
                total = jnp.dot(hid[zb, c], dw[:, cs], preferred_element_type=jnp.float32)
                for i in (0, 1):
                    part[zb, i, rs, cs] = total[i * piece_rows:(i + 1) * piece_rows].astype(
                        jnp.bfloat16)
                trade_far(zb, c, h).start()
            for h in (0, 1):
                rs, cs = corner(c, h)
                trade_far(zb, c, h).wait()

                @pl.when(at_end)
                def _():
                    red[zb, rs, cs] = both_far(zb, rs, cs).astype(jnp.bfloat16)
                    give_comb(t, zb, c, h).start()

    def combine(t):
        zb = far_block(t)

        @pl.when((z > 0) & (z < GROUP - 1))
        def _():
            @pl.loop(0, 2)
            def _(c):
                for h in (0, 1):
                    rs, cs = corner(c, h)
                    give_comb(t, zb, c, h).wait_recv()
                    red[zb, rs, cs] = (both_far(zb, rs, cs)
                                       + comb[t, rs, cs].astype(jnp.float32)).astype(jnp.bfloat16)
                    give_far(zb, c, h).start()

    send_far(0)
    send_far(1)
    combine(0)

    @pl.loop(0, 2)
    def _(c):
        expand(z, c)

    @pl.loop(0, GROUP)
    def _(g):
        lower(z, g)

    combine(1)

    @pl.loop(0, GROUP)
    def _(g):
        trade(z, g).wait()

    for c in (0, 1):
        for h in (0, 1):
            give_far(far, c, h).wait_recv()

    @pl.loop(0, GROUP)
    def _(g):
        at = span(g, gcols)
        give(mate_z, g).wait_recv()
        total = both(z, at) + got[0, :, at].astype(jnp.float32) + got[1, :, at].astype(jnp.float32)
        out_ref[:, at] = (mid[:, at] + 0.5 * total).astype(jnp.bfloat16)

    for d in range(1, GROUP):
        zb = (z + d) % GROUP
        for a in range(7):
            z_copy(a, zb).wait_send()
        remote(att.at[zb], arr.at[z], a_send.at[zb], a_recv.at[z], there(zb)).wait_send()

        @pl.loop(0, GROUP)
        def _(g):
            give(zb, g).wait_send()

    for a in range(6):
        for e in neighbours:
            p_own(a, e).wait_send()
            for d in range(1, GROUP):
                p_copy(a, (z + d) % GROUP, e).wait_send()
    for c in (0, 1):
        share(z, c).wait_send()
        for side in (0, 1):
            @pl.when(onward(side))
            def _():
                relay(z, side, c, o_send.at[side, c]).wait_send()
        for d in range(1, GROUP):
            share((z + d) % GROUP, c).wait_send()
            for side in (0, 1):
                zb = z - d if side == 0 else z + d

                @pl.when((zb >= 0) & (zb < GROUP) & onward(side))
                def _():
                    relay(zb, side, c, n_send.at[zb, c]).wait_send()


def grouped(
    sp, resid, queries, keys, values, log_gates, documents, out_weight, attn_gain, mlp_gain,
    gate_weight, up_weight, down_weight,
):
    rows, ff = keys.shape[0], gate_weight.shape[1] // GROUP
    half, d_model = resid.shape
    tokens = rows * sp
    qcols = queries.shape[1] // GROUP
    rank = qcols // HD
    bf, f32 = jnp.bfloat16, jnp.float32
    dma = pltpu.SemaphoreType.DMA
    return pl.pallas_call(
        layer_kernel,
        out_shape=jax.ShapeDtypeStruct(resid.shape, bf),
        in_specs=[VMEM] * 5 + [ANY] * 2 + [VMEM] * 2 + [ANY] * 3,
        out_specs=VMEM,
        scratch_shapes=[
            pltpu.VMEM(out_weight.shape, bf),
            pltpu.VMEM(resid.shape, bf),
            pltpu.VMEM((tokens, HD), bf),
            pltpu.VMEM((tokens, HD), bf),
            pltpu.VMEM((sp, 1, rows), jnp.int32),
            pltpu.VMEM((GROUP, rows, qcols), bf),
            pltpu.VMEM((rank, tokens, 128), f32),
            pltpu.VMEM((d_model, ff), bf),
            pltpu.VMEM((d_model, ff), bf),
            pltpu.VMEM((ff, d_model), bf),
            pltpu.VMEM((GROUP, rows, qcols), bf),
            pltpu.VMEM((GROUP, rows, qcols), bf),
            pltpu.VMEM((2, half, d_model), bf),
            pltpu.VMEM((half, d_model), bf),
            pltpu.VMEM((half, d_model), f32),
            pltpu.VMEM((GROUP, 2, half, d_model), bf),
            pltpu.VMEM((GROUP, 2, half, ff), bf),
            pltpu.VMEM((GROUP, 2, half, d_model), bf),
            pltpu.VMEM((GROUP, half, d_model), bf),
            pltpu.VMEM((GROUP, half, d_model), bf),
            pltpu.VMEM((2, half, d_model), bf),
            pltpu.VMEM((2, half, d_model), bf),
            dma((7, GROUP)), dma((7, GROUP)), dma((6, GROUP, 3)), dma((6, GROUP, 3)), dma((7,)),
            dma((2,)),
            dma((GROUP,)), dma((GROUP,)), dma, dma,
            dma((2, 2)), dma((GROUP, 2)), dma((GROUP, 2)), dma((GROUP, 2)), dma((GROUP, 2)),
            dma((GROUP, GROUP)), dma((GROUP, GROUP)), dma((GROUP, GROUP)), dma((2, GROUP)),
            dma((2, GROUP)),
        ],
        compiler_params=pltpu.CompilerParams(
            collective_id=0, has_side_effects=True, vmem_limit_bytes=62 * 1024 * 1024),
    )(queries, keys, values, documents[None, :], log_gates,
      out_weight, resid, attn_gain[None, :], mlp_gain[None, :], gate_weight, up_weight,
      down_weight)


def solution(mesh):
    placed = (
        P(("sp", "tp"), None),
        P("sp", "tp"),
        P("sp", "tp"),
        P("sp", "tp"),
        P("tp", None),
        P("sp"),
        P("tp", None),
        P(),
        P(),
        P("sp", "tp"),
        P("sp", "tp"),
        P("tp", "sp"),
    )
    sp, tp = mesh.shape["sp"], mesh.shape["tp"]

    def layer(*args):
        kv_dev = args[2].shape[1] // HD
        fits = tp == 2 and sp == GROUP * PLANE and kv_dev == GROUP
        return grouped(sp, *args) if fits else local(*args)

    return jax.shard_map(
        layer, mesh=mesh, in_specs=placed, out_specs=P(("sp", "tp"), None), check_vma=False
    )
```
